32 devices in a mesh: sp: 8 (over z, x), dp: 4 (over y, core).
Axes of the slice: x: 2, y: 2, z: 4, core: 2. Of those that a mesh axis runs over, the one named last changes fastest.
Arguments:
- query_rows: bfloat16 [4, 1024, 2048], P('dp', 'sp'), may hold values from -6 to 6
- key_rows: bfloat16 [4, 1024, 2048], P('dp', 'sp'), may hold values from -6 to 6
- value_rows: bfloat16 [4, 1024, 2048], P('dp', 'sp'), may hold values from -6 to 6
- decay_low: bfloat16 [4, 1024, 128], P('dp', 'sp'), may hold values from -5 to 5
- rate_low: bfloat16 [4, 1024, 128], P('dp', 'sp'), may hold values from -4 to 4
- decay_up: bfloat16 [128, 2048], replicated, may hold values from -0.5 to 0.5
- rate_up: bfloat16 [128, 2048], replicated, may hold values from -0.5 to 0.5
- decay_base: float32 [2048], replicated, may hold values from -12 to -2
- norm_gain: float32 [2048], replicated, may hold values from 0.1 to 1.9
- out_weight: bfloat16 [2048, 2048], P(None, 'dp'), may hold values from -0.125 to 0.125
Outputs:
- layer_out: bfloat16 [4, 1024, 2048], P('dp', 'sp')
The draws below stay inside these ranges and needn't reach their ends.
All inputs are finite; a program needn't handle non-finite values.
Results may differ from the reference program's by a relative error of at most 0.005.
Values may be sent and summed in bfloat16 or wider, within the bound.
A program may use at most 128 MiB of HBM per device.

```python
import jax
import jax.numpy as jnp
from jax import lax

D = 2048
HEADS = 32
HEAD = 64
LOW = 128
TOK_DEV = 128
WIDTH = 2048
LENGTH = 1024
BATCH = 4


def draw_decay_low(key, part):
    noise = jnp.clip(jax.random.normal(jax.random.fold_in(key, 11), (BATCH, LENGTH, LOW), jnp.float32), -4.0, 4.0)
    offsets = jax.random.uniform(jax.random.fold_in(key, 12), (BATCH, LENGTH // TOK_DEV, 1), jnp.float32, minval=-1.0, maxval=1.0)
    total = noise + jnp.repeat(offsets, TOK_DEV, axis=1)
    return jnp.clip(total, -5.0, 5.0).astype(jnp.bfloat16)


def draw_decay_base(key, part):
    picks = jax.random.randint(jax.random.fold_in(key, 21), (HEADS, 1), 0, 16)
    quick = picks < 8
    slow_rate = jax.random.uniform(jax.random.fold_in(key, 22), (HEADS, HEAD), jnp.float32, minval=0.2, maxval=1.0) / LENGTH
    quick_rate = jax.random.uniform(jax.random.fold_in(key, 23), (HEADS, HEAD), jnp.float32, minval=0.01, maxval=0.033)
    chosen = jnp.where(quick, quick_rate, slow_rate)
    return jnp.clip(jnp.log(chosen) + 0.5, -12.0, -2.0).reshape(WIDTH).astype(jnp.float32)


def block_levels(key, extent, pieces, least, top_value):
    level = 1.0
    for dim, parts in pieces:
        heights = jax.random.uniform(jax.random.fold_in(jax.random.fold_in(key, 6), dim), (parts,), jnp.float32, least / len(pieces), top_value / len(pieces))
        level = level * jnp.repeat(jnp.exp(heights), extent[dim] // parts).reshape((-1,) + (1,) * (len(extent) - 1 - dim))
    return level


def gaussian(stream_key, dims, deviation, reach, cuts=(), held_as=jnp.bfloat16):
    values = deviation * jax.random.normal(stream_key, dims, jnp.float32)
    if cuts:
        values = values * block_levels(stream_key, dims, cuts, -0.22, 0.18)
    return jnp.clip(values, -reach, reach).astype(held_as)


def setup_inputs(seed: int = 0) -> dict:
    splits = jax.random.split(jax.random.key(seed), 11)
    query_rows = gaussian(splits[0], (BATCH, LENGTH, WIDTH), 1.0, 6.0, ((0, 4), (1, 8)))
    key_rows = gaussian(splits[1], (BATCH, LENGTH, WIDTH), 1.0, 6.0, ((0, 4), (1, 8)))
    value_rows = gaussian(splits[2], (BATCH, LENGTH, WIDTH), 1.0, 6.0, ((0, 4), (1, 8)))
    decay_low = draw_decay_low(jax.random.fold_in(splits[10], 71), 0)
    rate_low = gaussian(splits[4], (BATCH, LENGTH, LOW), 1.0, 4.0, ((0, 4), (1, 8)))
    decay_up = gaussian(splits[5], (LOW, WIDTH), LOW ** -0.5, 0.5)
    rate_up = gaussian(splits[6], (LOW, WIDTH), LOW ** -0.5, 0.5)
    decay_base = draw_decay_base(jax.random.fold_in(splits[10], 71), 0)
    norm_gain = jnp.clip(1.0 + 0.18 * jax.random.normal(splits[8], (WIDTH,), jnp.float32), 0.1, 1.9)
    out_weight = gaussian(splits[9], (WIDTH, D), WIDTH ** -0.5, 0.125, ((1, 4),))
    return {"query_rows": query_rows, "key_rows": key_rows, "value_rows": value_rows, "decay_low": decay_low, "rate_low": rate_low, "decay_up": decay_up, "rate_up": rate_up, "decay_base": decay_base, "norm_gain": norm_gain, "out_weight": out_weight}


HIGHEST = lax.Precision.HIGHEST

def reference(query_rows, key_rows, value_rows, decay_low, rate_low, decay_up, rate_up, decay_base, norm_gain, out_weight):
    heads = query_rows.shape[2] // HEAD

    def one_sequence(inputs):
        reads, keyed, valued, low_decay, low_rate = inputs
        positions = reads.shape[0]
        squashed = jnp.tanh(low_decay.astype(jnp.float32)).astype(jnp.bfloat16)
        decay_pre = (decay_base + jnp.dot(squashed, decay_up, preferred_element_type=jnp.float32)).astype(jnp.bfloat16)
        rate_pre = jnp.dot(low_rate, rate_up, preferred_element_type=jnp.float32).astype(jnp.bfloat16)
        log_decay = -jnp.exp(-jax.nn.softplus(-decay_pre.astype(jnp.float32)) - 0.5)
        rate = jax.nn.sigmoid(rate_pre.astype(jnp.float32))
        head_shape = (positions, heads, HEAD)
        query_heads = reads.astype(jnp.float32).reshape(head_shape)
        key_heads = keyed.astype(jnp.float32).reshape(head_shape)
        value_heads = valued.astype(jnp.float32).reshape(head_shape)
        decay_heads = jnp.exp(log_decay).reshape(head_shape)
        unit_keys = key_heads * lax.rsqrt(1.0 + lax.optimization_barrier(jnp.sum(key_heads * key_heads, axis=-1, keepdims=True)))
        erase = unit_keys * rate.reshape(head_shape)

        def advance(state, inputs_now):
            query_now, decay_now, key_now, value_now, unit_now, erase_now = inputs_now
            removed = jnp.einsum('hvk,hk->hv', state, unit_now, precision=HIGHEST)
            state = state * decay_now[:, None, :] - removed[:, :, None] * erase_now[:, None, :] + value_now[:, :, None] * key_now[:, None, :]
            return (state, jnp.einsum('hvk,hk->hv', state, query_now, precision=HIGHEST))
        initial = jnp.zeros((heads, HEAD, HEAD), jnp.float32)
        _, readout = lax.scan(advance, initial, (query_heads, decay_heads, key_heads, value_heads, unit_keys, erase))
        average = lax.optimization_barrier(jnp.mean(readout, axis=-1, keepdims=True))
        centred = readout - average
        variance = lax.optimization_barrier(jnp.mean(centred * centred, axis=-1, keepdims=True))
        normed = (centred * lax.rsqrt(variance + 1.0)).reshape(positions, heads * HEAD)
        mix = (normed * norm_gain).astype(jnp.bfloat16)
        return jnp.dot(mix, out_weight, preferred_element_type=jnp.float32).astype(jnp.bfloat16)
    return lax.map(one_sequence, (query_rows, key_rows, value_rows, decay_low, rate_low))
```

```python
import functools
import math

import jax
import jax.numpy as jnp
from jax import lax
from jax.experimental import pallas as pl
from jax.experimental.pallas import tpu as pltpu
from jax.sharding import PartitionSpec as P

HEAD = 64
PAIR = 2 * HEAD
WIDE = 4

F32 = jnp.float32
BF16 = jnp.bfloat16


def mm(left, right):
    return lax.dot_general(left, right, (((1,), (0,)), ((), ())), preferred_element_type=F32)


def mm_nt(left, right):
    return lax.dot_general(left, right, (((1,), (1,)), ((), ())), preferred_element_type=F32)


def mm_tn(left, right):
    return lax.dot_general(left, right, (((0,), (0,)), ((), ())), preferred_element_type=F32)


def split(x):
    high = x.astype(BF16)
    return high, (x - high.astype(F32)).astype(BF16)


def mm_ab(left, right, form=mm):
    return form(left[0], right[0]) + form(left[0], right[1]) + form(left[1], right[0])


def beside(*parts):
    return jnp.concatenate(parts, axis=1)


def below(*parts):
    return jnp.concatenate(parts, axis=0)


def swap(x):
    return pltpu.roll(x, HEAD, 1)


def iota(shape, dim):
    return lax.broadcasted_iota(jnp.int32, shape, dim)


def first_half(shape):
    return iota(shape, len(shape) - 1) < HEAD


def stack_pair(x):
    here = lax.rem(iota(x.shape, 1), PAIR) < HEAD
    zero = jnp.zeros_like(x)
    return jnp.concatenate([jnp.where(here, x, zero), jnp.where(here, zero, x)], axis=0)


def head_ones(scale):
    row = iota((PAIR, PAIR), 0)
    col = iota((PAIR, PAIR), 1)
    return jnp.where(row // HEAD == col // HEAD, F32(scale), F32(0.0)).astype(BF16)


def head_sum(x, ones):
    return mm(beside(*split(x)), below(ones, ones))


def solve(parts, size):
    row = iota((size, size), 0)
    col = iota((size, size), 1)
    whole = [beside(z, y) for z, y in parts]
    block = 1
    while block < size:
        last = 2 * block == size
        pick = (row // (2 * block) == col // (2 * block)) & (row // block != col // block)
        fine = block % 16 != 0
        spans = [(0, size)] if fine else [(r + block, r + 2 * block) for r in range(0, size, 2 * block)]
        found = []
        for x in whole:
            high, low = split(x)
            move = jnp.where(pick, high[:, :size], jnp.zeros_like(high[:, :size]))
            move = move if fine else below(*[move[a:b] for a, b in spans])
            if last:
                x, high, low = x[:, size:], high[:, size:], low[:, size:]
            step = mm(beside(move, move), below(high, low))
            if fine:
                found.append(x - step)
            else:
                rows = []
                for i, (a, b) in enumerate(spans):
                    rows += [x[a - block : a], x[a:b] - step[i * block : (i + 1) * block]]
                found.append(below(*rows))
        whole = found
        block *= 2
    return whole


def gates(squashed, rate_low, decay_up, rate_up, base):
    decay_pre = (base + mm(squashed, decay_up)).astype(BF16).astype(F32)
    rate_pre = mm(rate_low, rate_up).astype(BF16).astype(F32)
    log_decay = -math.exp(-0.5) / (1.0 + jnp.exp(-decay_pre))
    rate = 1.0 / (1.0 + jnp.exp(-rate_pre))
    return log_decay, rate


def pair_grid(left, right):
    return mm_nt(beside(*left), beside(right[0], right[0])) + mm_nt(left[0], right[1])


def make_pairs(pairs):
    size = pairs[0][0].shape[0]
    middle = size // 2
    row = iota((size, size), 0)
    col = iota((size, size), 1)
    strict = row > col
    within = row >= col
    upto = jnp.where(within, F32(1.0), F32(0.0)).astype(BF16)
    upto = beside(upto, upto)
    ones = head_ones(1.0)
    half = first_half((size, PAIR))
    runs = [mm(upto, below(*split(p[3]))) for p in pairs]
    sums = []
    for p in pairs:
        k = p[1].astype(F32)
        sums.append(mm((k * k).astype(BF16), ones))
    made = []
    for (q, k, v, log_decay, rate), running, total in zip(pairs, runs, sums):
        k = k.astype(F32)
        centre = running[middle : middle + 1]
        final = running[size - 1 :]
        behind = jnp.exp(centre - running)
        unit = k * lax.rsqrt(1.0 + total)
        erase_from = unit * jnp.exp(running - log_decay - centre)
        read_from = q.astype(F32) * jnp.exp(running - centre)
        key_to = k * behind
        erase_to = unit * rate * behind
        made.append((erase_from, read_from, key_to, erase_to, centre, final))
    grids = []
    for erase_from, read_from, key_to, erase_to, _, _ in made:
        left = split(below(stack_pair(erase_from), stack_pair(read_from)))
        grids.append(pair_grid(left, split(below(key_to, erase_to))))

    def part(grid, i, j, keep):
        return jnp.where(keep, grid[i * size : (i + 1) * size, j * size : (j + 1) * size], 0.0)

    stacked = [stack_pair(p[2]) for p in pairs]
    parts = []
    for grid, values, (erase_from, _, _, _, centre, _) in zip(grids, stacked, made):
        keys = split(beside(part(grid, 0, 0, strict), part(grid, 1, 0, strict)))
        carried = mm(keys[0], values) + mm(keys[1], values)
        erase = erase_from * jnp.exp(centre)
        parts.append((part(grid, 0, 1, strict), jnp.where(half, erase, swap(carried))))
        parts.append((part(grid, 1, 1, strict), jnp.where(half, swap(erase), carried)))
    solved = solve(parts, size)
    row2 = iota((PAIR, PAIR), 0)
    col2 = iota((PAIR, PAIR), 1)
    half2 = first_half((HEAD, PAIR))
    fold = lambda x: jnp.where(half2, x[:HEAD], x[HEAD:])
    out = []
    for i, (p, grid, values, (_, read_from, key_to, erase_to, centre, final)) in enumerate(
        zip(pairs, grids, stacked, made)
    ):
        a, b = solved[2 * i], solved[2 * i + 1]
        both = split(beside(jnp.where(half, a, swap(b)), jnp.where(half, swap(a), b)))
        at_end = jnp.exp(final - centre)
        erase_end = split(erase_to * at_end)
        key_end = split(key_to * at_end)
        moved = mm_tn(below(*erase_end), below(both[0], both[0])) + mm_tn(erase_end[0], both[1])
        gained = mm_tn(below(*key_end), below(p[2], p[2]))
        read_keys = split(beside(part(grid, 2, 0, within), part(grid, 3, 0, within)))
        read_erase = split(beside(part(grid, 2, 1, within), part(grid, 3, 1, within)))
        here = mm(read_keys[0], values) + mm(read_keys[1], values)
        taken = mm_ab(read_erase, [stack_pair(x) for x in both])
        decay = jnp.broadcast_to(jnp.exp(final), (PAIR, PAIR))
        transfer = jnp.where(row2 == col2, decay, 0.0) - moved[:, :PAIR]
        added = gained - moved[:, PAIR:]
        read_state = read_from * jnp.exp(centre) - taken[:, :PAIR]
        out.append(
            split(below(fold(transfer), read_state))
            + (below(fold(added), here - taken[:, PAIR:]),)
        )
    return out


def normed(readout, ones):
    centred = readout - head_sum(readout, ones)
    variance = head_sum(centred * centred, ones)
    return centred * lax.rsqrt(variance + 1.0)


def fused_kernel(devices, columns, wide, lanes, pieces, q_ref, k_ref, v_ref, low_ref, rate_ref,
                 dup_ref, rup_ref, base_ref, gain_ref, weight_ref, out_ref, weights, maps_ref,
                 adds_ref, mix_ref, start_buf, end_buf, own_sem, near_sem, far_send, far_recv,
                 pass_send, pass_recv, send_sem, recv_sem):
    me = lax.axis_index("sp")
    mine = lax.axis_index("dp")
    partner = mine + 1 - 2 * lax.rem(mine, 2)
    width = q_ref.shape[1]
    groups = width // lanes
    blocks = width // wide
    each = wide // lanes
    others = columns // 2 - 1
    cols = weight_ref.shape[1]
    piece = weight_ref.shape[0] // pieces
    has_left = me > 0
    has_right = me < devices - 1
    barrier = pltpu.get_barrier_semaphore()

    def greet(where):
        pl.semaphore_signal(barrier, inc=1, device_id=where, device_id_type=pl.DeviceIdType.MESH)

    def ahead_of(j):
        return lax.rem(mine + 2 * (j + 1), columns)

    def behind_of(j):
        return lax.rem(mine + columns - 2 * (j + 1), columns)

    def remote(src, dst, send, recv, where):
        return pltpu.make_async_remote_copy(
            src_ref=src, dst_ref=dst, send_sem=send, recv_sem=recv,
            device_id=where, device_id_type=pl.DeviceIdType.MESH,
        )

    greet({"dp": partner})
    for j in range(others):
        greet({"dp": ahead_of(j)})

    @pl.when(has_left)
    def _():
        greet({"sp": me - 1})

    @pl.when(has_right)
    def _():
        greet({"sp": me + 1})

    own = pltpu.make_async_copy(weight_ref, weights.at[mine], own_sem)
    own.start()
    pl.semaphore_wait(
        barrier, 1 + others + jnp.minimum(me, 1) + jnp.minimum(devices - 1 - me, 1)
    )

    def rows(c):
        return pl.ds(c * piece, piece)

    def far(j, c):
        return remote(
            weight_ref.at[rows(c)], weights.at[mine, rows(c)],
            far_send.at[j, c], far_recv.at[j, c], {"dp": ahead_of(j)},
        )

    def passed(j, c):
        return remote(
            weights.at[behind_of(j), rows(c)], weights.at[behind_of(j), rows(c)],
            pass_send.at[j, c], pass_recv.at[j, c], {"dp": partner},
        )

    near = remote(weight_ref, weights.at[mine], near_sem.at[0], near_sem.at[1], {"dp": partner})
    for j in range(others):
        for c in range(pieces):
            far(j, c).start()
    near.start()

    def forward(c):
        for j in range(others):
            far(j, c).wait_recv()
            passed(j, c).start()

    def lanes_of(g, size):
        return pl.ds(pl.multiple_of(g * size, size), size)

    def cut(x, i):
        return x[:, i * PAIR : (i + 1) * PAIR]

    def make(b):
        at = lanes_of(b, wide)
        squashed = jnp.tanh(low_ref[...].astype(F32)).astype(BF16)
        log_decay, rate = gates(
            squashed, rate_ref[...], dup_ref[:, at], rup_ref[:, at], base_ref[:, at]
        )
        q, k, v = q_ref[:, at], k_ref[:, at], v_ref[:, at]
        made = make_pairs(
            [tuple(cut(x, i) for x in (q, k, v, log_decay, rate)) for i in range(wide // PAIR)]
        )
        high, low, adds = [beside(*part) for part in zip(*made)]
        maps_ref[0, :, at], maps_ref[1, :, at], adds_ref[:, at] = high, low, adds

    def copy(g):
        return remote(
            end_buf.at[g], start_buf.at[g], send_sem.at[g], recv_sem.at[g],
            {"sp": lax.rem(me + 1, devices)},
        )

    mean_ones = head_ones(1.0 / HEAD)

    def advance(g):
        at = lanes_of(g, lanes)

        @pl.when(has_left)
        def _():
            copy(g).wait_recv()

        start = start_buf[g]
        states = [stack_pair(cut(start, i)) for i in range(lanes // PAIR)]
        states = [below(x, x) for x in states]

        def apply(a, b):
            high, low, adds = maps_ref[0, a:b, at], maps_ref[1, a:b, at], adds_ref[a:b, at]
            return [
                mm(beside(cut(high, i), cut(low, i)), x) + cut(adds, i)
                for i, x in enumerate(states)
            ]

        end_buf[g] = beside(*apply(0, HEAD)).astype(BF16)

        @pl.when(has_right)
        def _():
            copy(g).start()

        readouts = apply(HEAD, maps_ref.shape[1])
        mix = beside(*[normed(x, mean_ones) for x in readouts])
        mix_ref[:, at] = (mix * gain_ref[:, at]).astype(BF16)

    @pl.when(jnp.logical_not(has_left))
    def _():
        start_buf[...] = jnp.zeros_like(start_buf)

    def slot(s, carry):
        @pl.when(s < blocks)
        def _():
            make(s)

        @pl.when((s >= me) & (s < me + blocks))
        def _():
            for i in range(each):
                advance((s - me) * each + i)

        return carry

    lax.fori_loop(0, blocks + devices - 1, slot, 0)
    for c in range(pieces):
        forward(c)

    def project(d):
        at = pl.ds(pl.multiple_of(d * cols, cols), cols)
        out_ref[:, at] = mm(mix_ref[...], weights[d]).astype(BF16)

    own.wait()
    project(mine)
    near.wait_recv()
    project(partner)
    for j in range(others):
        project(behind_of(j))
    for j in range(others):
        for c in range(pieces):
            passed(j, c).wait_recv()
        project(lax.rem(partner + columns - 2 * (j + 1), columns))

    near.wait_send()
    for j in range(others):
        for c in range(pieces):
            far(j, c).wait_send()
            passed(j, c).wait_send()

    @pl.when(has_right)
    def _():
        for g in range(groups):
            copy(g).wait_send()


def per_device(devices, columns, query_rows, key_rows, value_rows, decay_low, rate_low, decay_up,
               rate_up, decay_base, norm_gain, out_weight):
    q = query_rows[0]
    size, width = q.shape
    depth, cols = out_weight.shape
    wide = PAIR * math.gcd(width // PAIR, WIDE)
    lanes = PAIR * math.gcd(wide // PAIR, 2)
    groups = width // lanes
    pieces = 4
    others = columns // 2 - 1
    vmem = pl.BlockSpec(memory_space=pltpu.VMEM)
    dma = lambda *dims: pltpu.SemaphoreType.DMA(dims)
    out = pl.pallas_call(
        functools.partial(fused_kernel, devices, columns, wide, lanes, pieces),
        in_specs=[vmem] * 9 + [pl.BlockSpec(memory_space=pl.ANY)],
        out_specs=vmem,
        out_shape=jax.ShapeDtypeStruct((size, columns * cols), BF16),
        scratch_shapes=[
            pltpu.VMEM((columns, depth, cols), BF16),
            pltpu.VMEM((2, HEAD + size, width), BF16),
            pltpu.VMEM((HEAD + size, width), F32),
            pltpu.VMEM((size, width), BF16),
            pltpu.VMEM((groups, HEAD, lanes), BF16),
            pltpu.VMEM((groups, HEAD, lanes), BF16),
            pltpu.SemaphoreType.DMA,
            dma(2),
            dma(others, pieces),
            dma(others, pieces),
            dma(others, pieces),
            dma(others, pieces),
            dma(groups),
            dma(groups),
        ],
        compiler_params=pltpu.CompilerParams(collective_id=0, has_side_effects=True),
        name="fused_mixer",
    )(
        q, key_rows[0], value_rows[0], decay_low[0], rate_low[0], decay_up, rate_up,
        decay_base[None], norm_gain[None], out_weight,
    )
    return out[None]


def solution(mesh):
    in_specs = (
        P("dp", "sp", None),
        P("dp", "sp", None),
        P("dp", "sp", None),
        P("dp", "sp", None),
        P("dp", "sp", None),
        P(),
        P(),
        P(),
        P(),
        P(None, "dp"),
    )
    return jax.shard_map(
        functools.partial(per_device, mesh.shape["sp"], mesh.shape["dp"]),
        mesh=mesh, in_specs=in_specs, out_specs=P("dp", "sp", None), check_vma=False,
    )
```

```python
import functools
import math

import jax
import jax.numpy as jnp
from jax import lax
from jax.experimental import pallas as pl
from jax.experimental.pallas import tpu as pltpu
from jax.sharding import PartitionSpec as P

HEAD = 64
PAIR = 2 * HEAD
WIDE = 4

F32 = jnp.float32
BF16 = jnp.bfloat16


def mm(left, right):
    return lax.dot_general(left, right, (((1,), (0,)), ((), ())), preferred_element_type=F32)


def mm_nt(left, right):
    return lax.dot_general(left, right, (((1,), (1,)), ((), ())), preferred_element_type=F32)


def mm_tn(left, right):
    return lax.dot_general(left, right, (((0,), (0,)), ((), ())), preferred_element_type=F32)


def split(x):
    high = x.astype(BF16)
    return high, (x - high.astype(F32)).astype(BF16)


def mm_ab(left, right, form=mm):
    return form(left[0], right[0]) + form(left[0], right[1]) + form(left[1], right[0])


def beside(*parts):
    return jnp.concatenate(parts, axis=1)


def below(*parts):
    return jnp.concatenate(parts, axis=0)


def swap(x):
    return pltpu.roll(x, HEAD, 1)


def iota(shape, dim):
    return lax.broadcasted_iota(jnp.int32, shape, dim)


def first_half(shape):
    return iota(shape, len(shape) - 1) < HEAD


def stack_pair(x):
    here = lax.rem(iota(x.shape, 1), PAIR) < HEAD
    zero = jnp.zeros_like(x)
    return jnp.concatenate([jnp.where(here, x, zero), jnp.where(here, zero, x)], axis=0)


def head_ones(scale):
    row = iota((PAIR, PAIR), 0)
    col = iota((PAIR, PAIR), 1)
    return jnp.where(row // HEAD == col // HEAD, F32(scale), F32(0.0)).astype(BF16)


def head_sum(x, ones):
    return mm(beside(*split(x)), below(ones, ones))


def solve(parts, size):
    row = iota((size, size), 0)
    col = iota((size, size), 1)
    whole = [beside(z, y) for z, y in parts]
    block = 1
    while block < size:
        last = 2 * block == size
        pick = (row // (2 * block) == col // (2 * block)) & (row // block != col // block)
        fine = block % 16 != 0
        spans = [(0, size)] if fine else [(r + block, r + 2 * block) for r in range(0, size, 2 * block)]
        found = []
        for x in whole:
            high, low = split(x)
            move = jnp.where(pick, high[:, :size], jnp.zeros_like(high[:, :size]))
            move = move if fine else below(*[move[a:b] for a, b in spans])
            if last:
                x, high, low = x[:, size:], high[:, size:], low[:, size:]
            step = mm(beside(move, move), below(high, low))
            if fine:
                found.append(x - step)
            else:
                rows = []
                for i, (a, b) in enumerate(spans):
                    rows += [x[a - block : a], x[a:b] - step[i * block : (i + 1) * block]]
                found.append(below(*rows))
        whole = found
        block *= 2
    return whole


def gates(squashed, rate_low, decay_up, rate_up, base):
    decay_pre = (base + mm(squashed, decay_up)).astype(BF16).astype(F32)
    rate_pre = mm(rate_low, rate_up).astype(BF16).astype(F32)
    log_decay = -math.exp(-0.5) / (1.0 + jnp.exp(-decay_pre))
    rate = 1.0 / (1.0 + jnp.exp(-rate_pre))
    return log_decay, rate


def pair_grid(left, right):
    return mm_nt(beside(*left), beside(right[0], right[0])) + mm_nt(left[0], right[1])


def chunk_maps(pairs):
    size = pairs[0][0].shape[0]
    middle = size // 2
    row = iota((size, size), 0)
    col = iota((size, size), 1)
    strict = row > col
    upto = jnp.where(row >= col, F32(1.0), F32(0.0)).astype(BF16)
    upto = beside(upto, upto)
    ones = head_ones(1.0)
    half = first_half((size, PAIR))
    runs = [mm(upto, below(*split(p[2]))) for p in pairs]
    sums = []
    for p in pairs:
        k = p[0].astype(F32)
        sums.append(head_sum(k * k, ones))
    made = []
    for (k, v, log_decay, rate), running, total in zip(pairs, runs, sums):
        k = k.astype(F32)
        centre = running[middle : middle + 1]
        behind = jnp.exp(centre - running)
        unit = k * lax.rsqrt(1.0 + total)
        erase_from = unit * jnp.exp(running - log_decay - centre)
        made.append((erase_from, k * behind, unit * rate * behind, centre, running[size - 1 :]))
    grids = []
    keeps = []
    for erase_from, key_to, erase_to, _, _ in made:
        keeps.append(split(key_to) + split(erase_to))
        key_high, key_low, erase_high, erase_low = keeps[-1]
        right = below(key_high, erase_high), below(key_low, erase_low)
        grids.append(pair_grid(split(stack_pair(erase_from)), right))

    def part(grid, i, j):
        return jnp.where(
            strict, grid[i * size : (i + 1) * size, j * size : (j + 1) * size], 0.0
        )

    parts = []
    for p, grid, (erase_from, _, _, centre, _) in zip(pairs, grids, made):
        values = stack_pair(p[1])
        keys = split(beside(part(grid, 0, 0), part(grid, 1, 0)))
        carried = mm(keys[0], values) + mm(keys[1], values)
        erase = erase_from * jnp.exp(centre)
        parts.append((part(grid, 0, 1), jnp.where(half, erase, swap(carried))))
        parts.append((part(grid, 1, 1), jnp.where(half, swap(erase), carried)))
    solved = solve(parts, size)
    row2 = iota((PAIR, PAIR), 0)
    col2 = iota((PAIR, PAIR), 1)
    half2 = first_half((HEAD, PAIR))
    fold = lambda x: jnp.where(half2, x[:HEAD], x[HEAD:])
    out = []
    for i, (p, keep, running, (_, key_to, erase_to, centre, final)) in enumerate(
        zip(pairs, keeps, runs, made)
    ):
        a, b = solved[2 * i], solved[2 * i + 1]
        both = split(beside(jnp.where(half, a, swap(b)), jnp.where(half, swap(a), b)))
        at_end = jnp.exp(final - centre)
        erase_end = split(erase_to * at_end)
        key_end = split(key_to * at_end)
        moved = mm_tn(below(*erase_end), below(both[0], both[0])) + mm_tn(erase_end[0], both[1])
        gained = mm_tn(below(*key_end), below(p[1], p[1]))
        decay = jnp.broadcast_to(jnp.exp(final), (PAIR, PAIR))
        transfer = jnp.where(row2 == col2, decay, 0.0) - moved[:, :PAIR]
        added = gained - moved[:, PAIR:]
        halves = tuple(x[:, j : j + PAIR] for j in (0, PAIR) for x in both)
        out.append((fold(transfer), fold(added), running) + keep + halves)
    return out


def chunk_reads(pairs):
    size = pairs[0][0].shape[0]
    within = iota((size, size), 0) >= iota((size, size), 1)
    grids = []
    fronts = []
    for q, v, running, keep in pairs:
        centre = running[size // 2 : size // 2 + 1]
        read_from = q.astype(F32) * jnp.exp(running - centre)
        fronts.append(read_from * jnp.exp(centre))
        right = below(keep[0], keep[2]), below(keep[1], keep[3])
        grids.append(pair_grid(split(stack_pair(read_from)), right))
    out = []
    for (q, v, running, keep), grid, front in zip(pairs, grids, fronts):
        part = lambda i, j: jnp.where(
            within, grid[i * size : (i + 1) * size, j * size : (j + 1) * size], 0.0
        )
        read_keys = split(beside(part(0, 0), part(1, 0)))
        read_erase = split(beside(part(0, 1), part(1, 1)))
        values = stack_pair(v)
        here = mm(read_keys[0], values) + mm(read_keys[1], values)
        both = [stack_pair(beside(keep[i + 4], keep[i + 6])) for i in (0, 1)]
        taken = mm_ab(read_erase, both)
        out.append(split(front - taken[:, :PAIR]) + (here - taken[:, PAIR:],))
    return out


def normed(readout, ones):
    centred = readout - head_sum(readout, ones)
    variance = head_sum(centred * centred, ones)
    return centred * lax.rsqrt(variance + 1.0)


def fused_kernel(devices, columns, wide, pieces, q_ref, k_ref, v_ref, low_ref, rate_ref,
                 dup_ref, rup_ref, base_ref, gain_ref, weight_ref, out_ref, weights, own_ref,
                 running_ref, kept_ref, read_ref, here_ref, first_ref, first_add, both_ref, both_add,
                 mix_ref, give_buf, take_buf, start_buf, end_buf, own_sem, near_sem, far_send,
                 far_recv, side_send, side_recv, long_send, long_recv, pass_send, pass_recv,
                 give_send, give_recv, send_sem, recv_sem):
    me = lax.axis_index("sp")
    mine = lax.axis_index("dp")
    partner = mine + 1 - 2 * lax.rem(mine, 2)
    odd = lax.rem(me, 2)
    pair = me // 2
    side = me + 1 - 2 * odd
    long = me + 2 - 4 * lax.rem(pair, 2)
    width = q_ref.shape[1]
    blocks = width // wide
    chain = devices // 2
    others = columns // 2 - 1
    cols = weight_ref.shape[1]
    piece = weight_ref.shape[0] // (4 * pieces)
    has_left = pair > 0
    has_right = pair < chain - 1
    barrier = pltpu.get_barrier_semaphore()

    def greet(where):
        pl.semaphore_signal(barrier, inc=1, device_id=where, device_id_type=pl.DeviceIdType.MESH)

    def ahead_of(j):
        return lax.rem(mine + 2 * (j + 1), columns)

    def behind_of(j):
        return lax.rem(mine + columns - 2 * (j + 1), columns)

    def remote(src, dst, send, recv, where):
        return pltpu.make_async_remote_copy(
            src_ref=src, dst_ref=dst, send_sem=send, recv_sem=recv,
            device_id=where, device_id_type=pl.DeviceIdType.MESH,
        )

    greet({"dp": partner})
    greet({"sp": side})
    for j in range(others):
        greet({"dp": ahead_of(j)})

    @pl.when(has_left)
    def _():
        greet({"sp": me - 2})

    @pl.when(has_right)
    def _():
        greet({"sp": me + 2})

    own = pltpu.make_async_copy(weight_ref, weights.at[mine], own_sem)
    own.start()
    pl.semaphore_wait(
        barrier, 2 + others + jnp.minimum(pair, 1) + jnp.minimum(chain - 1 - pair, 1)
    )

    quarter = lax.rem(me, 4)
    side_quarter = quarter + 1 - 2 * odd
    long_quarter = lax.rem(quarter + 2, 4)
    last_quarter = 3 - quarter
    arrivals = (quarter, last_quarter, side_quarter, long_quarter)

    def rows(part, c):
        return pl.ds((part * pieces + c) * piece, piece)

    def far(j, part, c):
        at = rows(arrivals[part], c)
        return remote(
            weight_ref.at[at], weights.at[mine, at],
            far_send.at[j, part, c], far_recv.at[j, part, c], {"dp": ahead_of(j)},
        )

    def spread(j, c, send, recv, where):
        at = rows(quarter, c)
        spot = weights.at[behind_of(j), at]
        return remote(spot, spot, send.at[j, c], recv.at[j, c], {"sp": where})

    def aside(j, c):
        return spread(j, c, side_send, side_recv, side)

    def along(j, c):
        return spread(j, c, long_send, long_recv, long)

    def passed(j, part, c):
        spot = weights.at[behind_of(j), rows(arrivals[part], c)]
        return remote(
            spot, spot, pass_send.at[j, part, c], pass_recv.at[j, part, c], {"dp": partner},
        )

    near = remote(weight_ref, weights.at[mine], near_sem.at[0], near_sem.at[1], {"dp": partner})
    for part in range(2):
        for c in range(pieces):
            for j in range(others):
                far(j, part, c).start()
    near.start()

    def forward(part, c):
        for j in range(others):
            if part < 2:
                far(j, part, c).wait_recv()
            elif part == 2:
                aside(j, c).wait_recv()
            else:
                along(j, c).wait_recv()
            if part == 0:
                aside(j, c).start()
                along(j, c).start()
            passed(j, part, c).start()

    def lanes_of(g):
        return pl.ds(pl.multiple_of(g * wide, wide), wide)

    def cut(x, i):
        return x[:, i * PAIR : (i + 1) * PAIR]

    def cuts(x):
        return [cut(x, i) for i in range(wide // PAIR)]

    def give(b):
        return remote(
            give_buf.at[b], take_buf.at[b], give_send.at[b], give_recv.at[b], {"sp": side}
        )

    def copy(b):
        return remote(
            end_buf.at[b], start_buf.at[b], send_sem.at[b], recv_sem.at[b],
            {"sp": lax.rem(me + 2, devices)},
        )

    def make(b):
        at = lanes_of(b)
        squashed = jnp.tanh(low_ref[...].astype(F32)).astype(BF16)
        log_decay, rate = gates(
            squashed, rate_ref[...], dup_ref[:, at], rup_ref[:, at], base_ref[:, at]
        )
        pairs = list(zip(*map(cuts, (k_ref[:, at], v_ref[:, at], log_decay, rate))))
        parts = [beside(*part) for part in zip(*chunk_maps(pairs))]
        maps = below(parts[0], parts[1])
        own_ref[:, at] = maps
        give_buf[b] = maps.astype(BF16)
        running_ref[:, at] = parts[2]
        for i, part in enumerate(parts[3:]):
            kept_ref[i, :, at] = part
        give(b).start()

    def combine(b):
        at = lanes_of(b)
        give(b).wait_recv()
        own, taken = own_ref[:, at], take_buf[b].astype(F32)
        is_odd = iota(own.shape, 0) * 0 + odd == 1
        first, second = jnp.where(is_odd, taken, own), jnp.where(is_odd, own, taken)
        found = []
        for x, y in zip(cuts(first), cuts(second)):
            left = split(y[:HEAD])
            right = split(beside(stack_pair(x[:HEAD]), stack_pair(x[HEAD:])))
            found.append((mm_ab(left, right), y[HEAD:]))
        both = beside(*[x[:, :PAIR] for x, _ in found])
        added = beside(*[x[:, PAIR:] + y for x, y in found])
        both_ref[0, :, at], both_ref[1, :, at] = split(both)
        both_add[:, at] = added
        same = (iota((HEAD, wide), 1) % HEAD == iota((HEAD, wide), 0)).astype(F32)
        is_odd = is_odd[:HEAD]
        first_ref[0, :, at], first_ref[1, :, at] = split(jnp.where(is_odd, first[:HEAD], same))
        first_add[:, at] = jnp.where(is_odd, first[HEAD:], 0.0)

        @pl.when(jnp.logical_not(has_left) & has_right)
        def _():
            end_buf[b] = added.astype(BF16)
            copy(b).start()

    def apply(high, low, state):
        return mm(beside(high, low), below(state, state))

    def advance(b):
        at = lanes_of(b)
        copy(b).wait_recv()

        @pl.when(has_right)
        def _():
            high, low, start = both_ref[0, :, at], both_ref[1, :, at], start_buf[b]
            ends = [apply(h, l, stack_pair(x)) for h, l, x in zip(*map(cuts, (high, low, start)))]
            end_buf[b] = (beside(*ends) + both_add[:, at]).astype(BF16)
            copy(b).start()

    def prepare(b):
        at = lanes_of(b)
        kept = [cuts(kept_ref[j, :, at]) for j in range(kept_ref.shape[0])]
        keeps = list(zip(*kept))
        pairs = list(zip(*map(cuts, (q_ref[:, at], v_ref[:, at], running_ref[:, at])), keeps))
        high, low, here = [beside(*part) for part in zip(*chunk_reads(pairs))]
        read_ref[0, :, at], read_ref[1, :, at], here_ref[:, at] = high, low, here

    ones = head_ones(1.0 / HEAD)

    def read(b):
        at = lanes_of(b)
        high, low, start = first_ref[0, :, at], first_ref[1, :, at], start_buf[b]
        starts = [apply(h, l, stack_pair(x)) for h, l, x in zip(*map(cuts, (high, low, start)))]
        starts = [split(x + y) for x, y in zip(starts, cuts(first_add[:, at]))]
        high, low, here = read_ref[0, :, at], read_ref[1, :, at], here_ref[:, at]
        reads = []
        for h, l, x, (s_high, s_low) in zip(*map(cuts, (high, low, here)), starts):
            reads.append(apply(h, l, stack_pair(s_high)) + mm(h, stack_pair(s_low)) + x)
        centred = [x - head_sum(x, ones) for x in reads]
        spans = [head_sum(x * x, ones) for x in centred]
        mix = beside(*[x * lax.rsqrt(y + 1.0) for x, y in zip(centred, spans)])
        mix_ref[:, at] = (mix * gain_ref[:, at]).astype(BF16)

    @pl.when(jnp.logical_not(has_left))
    def _():
        start_buf[...] = jnp.zeros_like(start_buf)

    lag = jnp.maximum(pair - 1, 0)
    slots = 2 * blocks + max(chain - 2, 0)
    plan = [(2, [(0, 0)]), (3, [(0, 1)]), (5, [(0, 2)]), (6, [(2, 0), (3, 0)]), (7, [(0, 3), (2, 1), (3, 1)])]

    def slot(s, carry):
        @pl.when(s < blocks)
        def _():
            make(s)

        @pl.when(((s >= 1) & (s < blocks)) | (s == 2 * blocks - 1))
        def _():
            combine(jnp.minimum(s, blocks) - 1)

        b = s - blocks - lag
        live = (b >= 0) & (b < blocks)

        @pl.when(live & has_left)
        def _():
            advance(b)

        @pl.when((s >= blocks) & (s < 2 * blocks))
        def _():
            prepare(s - blocks)

        @pl.when(live)
        def _():
            read(b)

        for at, todo in plan:
            @pl.when(s == at)
            def _():
                for part, c in todo:
                    forward(part, c)

        return carry

    lax.fori_loop(0, slots, slot, 0)
    done = [x for _, todo in plan for x in todo]
    for c in range(pieces):
        for part in (0, 2, 3, 1):
            if (part, c) not in done:
                forward(part, c)

    def project(d):
        at = pl.ds(pl.multiple_of(d * cols, cols), cols)
        out_ref[:, at] = mm(mix_ref[...], weights[d]).astype(BF16)

    own.wait()
    project(mine)
    near.wait_recv()
    project(partner)
    for j in range(others):
        project(behind_of(j))
    for j in range(others):
        for part in range(4):
            for c in range(pieces):
                passed(j, part, c).wait_recv()
        project(lax.rem(partner + columns - 2 * (j + 1), columns))

    near.wait_send()
    for j in range(others):
        for part in range(4):
            for c in range(pieces):
                passed(j, part, c).wait_send()
        for c in range(pieces):
            aside(j, c).wait_send()
            along(j, c).wait_send()
            far(j, 0, c).wait_send()
            far(j, 1, c).wait_send()

    for b in range(blocks):
        give(b).wait_send()

    @pl.when(has_right)
    def _():
        for b in range(blocks):
            copy(b).wait_send()


def per_device(devices, columns, query_rows, key_rows, value_rows, decay_low, rate_low, decay_up,
               rate_up, decay_base, norm_gain, out_weight):
    q = query_rows[0]
    size, width = q.shape
    depth, cols = out_weight.shape
    wide = PAIR * math.gcd(width // PAIR, WIDE)
    blocks = width // wide
    pieces = 4
    others = columns // 2 - 1
    vmem = pl.BlockSpec(memory_space=pltpu.VMEM)
    dma = lambda *dims: pltpu.SemaphoreType.DMA(dims)
    out = pl.pallas_call(
        functools.partial(fused_kernel, devices, columns, wide, pieces),
        in_specs=[vmem] * 9 + [pl.BlockSpec(memory_space=pl.ANY)],
        out_specs=vmem,
        out_shape=jax.ShapeDtypeStruct((size, columns * cols), BF16),
        scratch_shapes=[
            pltpu.VMEM((columns, depth, cols), BF16),
            pltpu.VMEM((2 * HEAD, width), F32),
            pltpu.VMEM((size, width), F32),
            pltpu.VMEM((8, size, width), BF16),
            pltpu.VMEM((2, size, width), BF16),
            pltpu.VMEM((size, width), F32),
            pltpu.VMEM((2, HEAD, width), BF16),
            pltpu.VMEM((HEAD, width), F32),
            pltpu.VMEM((2, HEAD, width), BF16),
            pltpu.VMEM((HEAD, width), F32),
            pltpu.VMEM((size, width), BF16),
            pltpu.VMEM((blocks, 2 * HEAD, wide), BF16),
            pltpu.VMEM((blocks, 2 * HEAD, wide), BF16),
            pltpu.VMEM((blocks, HEAD, wide), BF16),
            pltpu.VMEM((blocks, HEAD, wide), BF16),
            pltpu.SemaphoreType.DMA,
            dma(2),
            dma(others, 2, pieces),
            dma(others, 2, pieces),
            dma(others, pieces),
            dma(others, pieces),
            dma(others, pieces),
            dma(others, pieces),
            dma(others, 4, pieces),
            dma(others, 4, pieces),
            dma(blocks),
            dma(blocks),
            dma(blocks),
            dma(blocks),
        ],
        compiler_params=pltpu.CompilerParams(collective_id=0, has_side_effects=True),
        name="fused_mixer",
    )(
        q, key_rows[0], value_rows[0], decay_low[0], rate_low[0], decay_up, rate_up,
        decay_base[None], norm_gain[None], out_weight,
    )
    return out[None]


def solution(mesh):
    in_specs = (
        P("dp", "sp", None),
        P("dp", "sp", None),
        P("dp", "sp", None),
        P("dp", "sp", None),
        P("dp", "sp", None),
        P(),
        P(),
        P(),
        P(),
        P(None, "dp"),
    )
    return jax.shard_map(
        functools.partial(per_device, mesh.shape["sp"], mesh.shape["dp"]),
        mesh=mesh, in_specs=in_specs, out_specs=P("dp", "sp", None), check_vma=False,
    )
```

```python
import functools
import math

import jax
import jax.numpy as jnp
from jax import lax
from jax.experimental import pallas as pl
from jax.experimental.pallas import tpu as pltpu
from jax.sharding import PartitionSpec as P

HEAD = 64
PAIR = 2 * HEAD
WIDE = 4
FINE = 16

F32 = jnp.float32
BF16 = jnp.bfloat16


def mm(left, right):
    return lax.dot_general(left, right, (((1,), (0,)), ((), ())), preferred_element_type=F32)


def mm_nt(left, right):
    return lax.dot_general(left, right, (((1,), (1,)), ((), ())), preferred_element_type=F32)


def mm_tn(left, right):
    return lax.dot_general(left, right, (((0,), (0,)), ((), ())), preferred_element_type=F32)


def split(x):
    high = x.astype(BF16)
    return high, (x - high.astype(F32)).astype(BF16)


def mm_ab(left, right, form=mm):
    return form(left[0], right[0]) + form(left[0], right[1]) + form(left[1], right[0])


def beside(*parts):
    return jnp.concatenate(parts, axis=1)


def below(*parts):
    return jnp.concatenate(parts, axis=0)


def swap(x):
    return pltpu.roll(x, HEAD, 1)


def iota(shape, dim):
    return lax.broadcasted_iota(jnp.int32, shape, dim)


def first_half(shape):
    return iota(shape, len(shape) - 1) < HEAD


def stack_pair(x):
    here = lax.rem(iota(x.shape, 1), PAIR) < HEAD
    zero = jnp.zeros_like(x)
    return jnp.concatenate([jnp.where(here, x, zero), jnp.where(here, zero, x)], axis=0)


def head_ones(scale):
    row = iota((PAIR, PAIR), 0)
    col = iota((PAIR, PAIR), 1)
    return jnp.where(row // HEAD == col // HEAD, F32(scale), F32(0.0)).astype(BF16)


def head_sum(x, ones):
    return mm(beside(*split(x)), below(ones, ones))


def crossed(x, y):
    zero = jnp.zeros_like(x)
    return below(beside(x, zero), beside(zero, y))


def solve(parts, size):
    row = iota((size, size), 0)
    col = iota((size, size), 1)
    whole = [beside(z, y) for z, y in parts]
    block = 1
    while block < size:
        last = 2 * block == size
        pick = (row // (2 * block) == col // (2 * block)) & (row // block != col // block)
        fine = block % 16 != 0
        spans = [(0, size)] if fine else [(r + block, r + 2 * block) for r in range(0, size, 2 * block)]
        found = []
        for x in whole:
            high, low = split(x)
            move = jnp.where(pick, high[:, :size], jnp.zeros_like(high[:, :size]))
            move = move if fine else below(*[move[a:b] for a, b in spans])
            if last:
                x, high, low = x[:, size:], high[:, size:], low[:, size:]
            step = mm(beside(move, move), below(high, low))
            if fine:
                found.append(x - step)
            else:
                rows = []
                for i, (a, b) in enumerate(spans):
                    rows += [x[a - block : a], x[a:b] - step[i * block : (i + 1) * block]]
                found.append(below(*rows))
        whole = found
        block *= 2
    return whole


def gates(squashed, rate_low, decay_up, rate_up, base):
    decay_pre = (base + mm(squashed, decay_up)).astype(BF16).astype(F32)
    rate_pre = mm(rate_low, rate_up).astype(BF16).astype(F32)
    log_decay = -math.exp(-0.5) / (1.0 + jnp.exp(-decay_pre))
    rate = 1.0 / (1.0 + jnp.exp(-rate_pre))
    return log_decay, rate


def pair_grid(left, right):
    return mm_nt(beside(*left), beside(right[0], right[0])) + mm_nt(left[0], right[1])


def chunk_maps(pairs):
    size = pairs[0][0].shape[0]
    middle = size // 2
    row = iota((size, size), 0)
    col = iota((size, size), 1)
    strict = row > col
    upto = jnp.where(row >= col, F32(1.0), F32(0.0)).astype(BF16)
    upto = beside(upto, upto)
    ones = head_ones(1.0)
    half = first_half((size, PAIR))
    runs = [mm(upto, below(*split(p[2]))) for p in pairs]
    means = head_ones(1.0 / HEAD)
    sums = []
    values = []
    for p in pairs:
        k = p[0].astype(F32)
        sums.append(head_sum(k * k, ones))
        values.append(split(p[1].astype(F32) - mm(p[1], means)))
    made = []
    for (k, v, log_decay, rate), running, total in zip(pairs, runs, sums):
        k = k.astype(F32)
        centre = running[middle : middle + 1]
        behind = jnp.exp(centre - running)
        unit = k * lax.rsqrt(1.0 + total)
        erase_from = unit * jnp.exp(running - log_decay - centre)
        made.append((erase_from, k * behind, unit * rate * behind, centre, running[size - 1 :]))
    grids = []
    keeps = []
    for erase_from, key_to, erase_to, _, _ in made:
        keeps.append(split(key_to) + split(erase_to))
        key_high, key_low, erase_high, erase_low = keeps[-1]
        right = below(key_high, erase_high), below(key_low, erase_low)
        grids.append(pair_grid(split(stack_pair(erase_from)), right))

    def part(grid, i, j):
        return jnp.where(
            strict, grid[i * size : (i + 1) * size, j * size : (j + 1) * size], 0.0
        )

    parts = []
    for v, grid, (erase_from, _, _, centre, _) in zip(values, grids, made):
        keys = split(beside(part(grid, 0, 0), part(grid, 1, 0)))
        carried = mm_ab(keys, [stack_pair(x) for x in v])
        erase = erase_from * jnp.exp(centre)
        parts.append((part(grid, 0, 1), jnp.where(half, erase, swap(carried))))
        parts.append((part(grid, 1, 1), jnp.where(half, swap(erase), carried)))
    solved = solve(parts, size)
    row2 = iota((PAIR, PAIR), 0)
    col2 = iota((PAIR, PAIR), 1)
    half2 = first_half((HEAD, PAIR))
    fold = lambda x: jnp.where(half2, x[:HEAD], x[HEAD:])
    out = []
    for i, (v, keep, running, (_, key_to, erase_to, centre, final)) in enumerate(
        zip(values, keeps, runs, made)
    ):
        a, b = solved[2 * i], solved[2 * i + 1]
        both = split(beside(jnp.where(half, a, swap(b)), jnp.where(half, swap(a), b)))
        at_end = jnp.exp(final - centre)
        erase_end = split(erase_to * at_end)
        key_end = split(key_to * at_end)
        moved = mm_tn(below(*erase_end), below(both[0], both[0])) + mm_tn(erase_end[0], both[1])
        gained = mm_tn(below(*key_end), below(v[0], v[0])) + mm_tn(key_end[0], v[1])
        decay = jnp.broadcast_to(jnp.exp(final), (PAIR, PAIR))
        transfer = jnp.where(row2 == col2, decay, 0.0) - moved[:, :PAIR]
        added = gained - moved[:, PAIR:]
        halves = tuple(x[:, j : j + PAIR] for j in (0, PAIR) for x in both)
        out.append((fold(transfer), fold(added), running) + keep + halves + v)
    return out


def chunk_reads(pairs):
    size = pairs[0][0].shape[0]
    within = iota((size, size), 0) >= iota((size, size), 1)
    grids = []
    fronts = []
    for q, running, keep in pairs:
        centre = running[size // 2 : size // 2 + 1]
        read_from = q.astype(F32) * jnp.exp(running - centre)
        fronts.append(read_from * jnp.exp(centre))
        right = below(keep[0], keep[2]), below(keep[1], keep[3])
        grids.append(pair_grid(split(stack_pair(read_from)), right))
    out = []
    for (_, _, keep), grid, front in zip(pairs, grids, fronts):
        part = lambda i, j: jnp.where(
            within, grid[i * size : (i + 1) * size, j * size : (j + 1) * size], 0.0
        )
        read_keys = split(beside(part(0, 0), part(1, 0)))
        read_erase = split(beside(part(0, 1), part(1, 1)))
        here = mm_ab(read_keys, [stack_pair(x) for x in keep[8:]])
        both = [stack_pair(beside(keep[i + 4], keep[i + 6])) for i in (0, 1)]
        taken = mm_ab(read_erase, both)
        out.append(split(front - taken[:, :PAIR]) + (here - taken[:, PAIR:],))
    return out


def fused_kernel(devices, columns, wide, pieces, q_hbm, k_hbm, v_hbm, low_hbm, rate_hbm,
                 dup_hbm, rup_hbm, base_hbm, gain_hbm, weight_ref, out_ref, q_ref, k_ref, v_ref,
                 low_ref, rate_ref, dup_ref, rup_ref, base_ref, gain_ref, in_sem, sums_ref, weights,
                 own_ref,
                 running_ref, kept_ref, read_ref, here_ref, first_ref, first_add, both_ref, both_add,
                 mix_ref, give_buf, take_buf, start_buf, end_buf, own_sem, near_sem, far_send,
                 far_recv, side_send, side_recv, long_send, long_recv, pass_send, pass_recv,
                 give_send, give_recv, send_sem, recv_sem):
    me = lax.axis_index("sp")
    mine = lax.axis_index("dp")
    partner = mine + 1 - 2 * lax.rem(mine, 2)
    odd = lax.rem(me, 2)
    pair = me // 2
    side = me + 1 - 2 * odd
    long = me + 2 - 4 * lax.rem(pair, 2)
    width = q_ref.shape[1]
    blocks = width // wide
    chain = devices // 2
    others = columns // 2 - 1
    cols = weight_ref.shape[1]
    piece = weight_ref.shape[0] // (4 * pieces)
    has_left = pair > 0
    has_right = pair < chain - 1
    barrier = pltpu.get_barrier_semaphore()

    def greet(where):
        pl.semaphore_signal(barrier, inc=1, device_id=where, device_id_type=pl.DeviceIdType.MESH)

    def ahead_of(j):
        return lax.rem(mine + 2 * (j + 1), columns)

    def behind_of(j):
        return lax.rem(mine + columns - 2 * (j + 1), columns)

    def remote(src, dst, send, recv, where):
        return pltpu.make_async_remote_copy(
            src_ref=src, dst_ref=dst, send_sem=send, recv_sem=recv,
            device_id=where, device_id_type=pl.DeviceIdType.MESH,
        )

    greet({"dp": partner})
    greet({"sp": side})
    for j in range(others):
        greet({"dp": ahead_of(j)})

    @pl.when(has_left)
    def _():
        greet({"sp": me - 2})

    @pl.when(has_right)
    def _():
        greet({"sp": me + 2})

    inputs = [
        (low_hbm, low_ref), (rate_hbm, rate_ref), (base_hbm, base_ref), (dup_hbm, dup_ref),
        (rup_hbm, rup_ref), (k_hbm, k_ref), (v_hbm, v_ref), (q_hbm, q_ref), (gain_hbm, gain_ref),
    ]
    loads = [pltpu.make_async_copy(x, y, in_sem.at[i]) for i, (x, y) in enumerate(inputs)]
    for load in loads:
        load.start()
    own = pltpu.make_async_copy(weight_ref, weights.at[mine], own_sem)
    own.start()
    pl.semaphore_wait(
        barrier, 2 + others + jnp.minimum(pair, 1) + jnp.minimum(chain - 1 - pair, 1)
    )

    quarter = lax.rem(me, 4)
    side_quarter = quarter + 1 - 2 * odd
    long_quarter = lax.rem(quarter + 2, 4)
    last_quarter = 3 - quarter
    arrivals = (quarter, last_quarter, side_quarter, long_quarter)

    def rows(part, c):
        return pl.ds((part * pieces + c) * piece, piece)

    def far(j, part, c):
        at = rows(arrivals[part], c)
        return remote(
            weight_ref.at[at], weights.at[mine, at],
            far_send.at[j, part, c], far_recv.at[j, part, c], {"dp": ahead_of(j)},
        )

    def spread(j, c, send, recv, where):
        at = rows(quarter, c)
        spot = weights.at[behind_of(j), at]
        return remote(spot, spot, send.at[j, c], recv.at[j, c], {"sp": where})

    def aside(j, c):
        return spread(j, c, side_send, side_recv, side)

    def along(j, c):
        return spread(j, c, long_send, long_recv, long)

    def passed(j, part, c):
        spot = weights.at[behind_of(j), rows(arrivals[part], c)]
        return remote(
            spot, spot, pass_send.at[j, part, c], pass_recv.at[j, part, c], {"dp": partner},
        )

    near = remote(weight_ref, weights.at[mine], near_sem.at[0], near_sem.at[1], {"dp": partner})
    for part in range(2):
        for c in range(pieces):
            for j in range(others):
                far(j, part, c).start()
    near.start()

    def forward(part, c):
        for j in range(others):
            if part < 2:
                far(j, part, c).wait_recv()
            elif part == 2:
                aside(j, c).wait_recv()
            else:
                along(j, c).wait_recv()
            if part == 0:
                along(j, c).start()
            passed(j, part, c).start()

    def lend(c):
        for j in range(others):
            aside(j, c).start()

    def lanes_of(g):
        return pl.ds(pl.multiple_of(g * wide, wide), wide)

    def cut(x, i):
        return x[:, i * PAIR : (i + 1) * PAIR]

    def cuts(x):
        return [cut(x, i) for i in range(wide // PAIR)]

    def give(b):
        return remote(
            give_buf.at[b], take_buf.at[b], give_send.at[b], give_recv.at[b], {"sp": side}
        )

    def copy(b):
        return remote(
            end_buf.at[b], start_buf.at[b], send_sem.at[b], recv_sem.at[b],
            {"sp": lax.rem(me + 2, devices)},
        )

    def make(b):
        at = lanes_of(b)
        squashed = jnp.tanh(low_ref[...].astype(F32)).astype(BF16)
        log_decay, rate = gates(
            squashed, rate_ref[...], dup_ref[:, at], rup_ref[:, at], base_ref[:, at]
        )
        pairs = list(zip(*map(cuts, (k_ref[:, at], v_ref[:, at], log_decay, rate))))
        parts = [beside(*part) for part in zip(*chunk_maps(pairs))]
        maps = below(parts[0], parts[1])
        own_ref[:, at] = maps
        give_buf[b] = maps.astype(BF16)
        running_ref[:, at] = parts[2]
        for i, part in enumerate(parts[3:]):
            kept_ref[i, :, at] = part
        give(b).start()

    def combine(b):
        at = lanes_of(b)
        give(b).wait_recv()
        own, taken = own_ref[:, at], take_buf[b].astype(F32)
        is_odd = iota(own.shape, 0) * 0 + odd == 1
        first, second = jnp.where(is_odd, taken, own), jnp.where(is_odd, own, taken)
        found = []
        for x, y in zip(cuts(first), cuts(second)):
            left = split(y[:HEAD])
            right = split(beside(stack_pair(x[:HEAD]), stack_pair(x[HEAD:])))
            found.append((mm_ab(left, right), y[HEAD:]))
        both = beside(*[x[:, :PAIR] for x, _ in found])
        added = beside(*[x[:, PAIR:] + y for x, y in found])
        both_ref[0, :, at], both_ref[1, :, at] = split(both)
        both_add[:, at] = added
        same = (iota((HEAD, wide), 1) % HEAD == iota((HEAD, wide), 0)).astype(F32)
        is_odd = is_odd[:HEAD]
        first_ref[0, :, at], first_ref[1, :, at] = split(jnp.where(is_odd, first[:HEAD], same))
        first_add[:, at] = jnp.where(is_odd, first[HEAD:], 0.0)

        @pl.when(jnp.logical_not(has_left) & has_right)
        def _():
            end_buf[b] = added.astype(BF16)
            copy(b).start()

    def apply(high, low, state):
        return mm(beside(high, low), below(state, state))

    def advance(b):
        at = lanes_of(b)
        copy(b).wait_recv()

        @pl.when(has_right)
        def _():
            high, low, start = both_ref[0, :, at], both_ref[1, :, at], start_buf[b]
            ends = [apply(h, l, stack_pair(x)) for h, l, x in zip(*map(cuts, (high, low, start)))]
            end_buf[b] = (beside(*ends) + both_add[:, at]).astype(BF16)
            copy(b).start()

    def prepare(b):
        at = lanes_of(b)
        kept = [cuts(kept_ref[j, :, at]) for j in range(kept_ref.shape[0])]
        keeps = list(zip(*kept))
        pairs = list(zip(*map(cuts, (q_ref[:, at], running_ref[:, at])), keeps))
        high, low, here = [beside(*part) for part in zip(*chunk_reads(pairs))]
        read_ref[0, :, at], read_ref[1, :, at], here_ref[:, at] = high, low, here

    ones = head_ones(1.0 / HEAD)

    def read(b):
        at = lanes_of(b)
        high, low, start = first_ref[0, :, at], first_ref[1, :, at], start_buf[b]
        starts = [apply(h, l, stack_pair(x)) for h, l, x in zip(*map(cuts, (high, low, start)))]
        starts = [split(x + y) for x, y in zip(starts, cuts(first_add[:, at]))]
        high, low, here = read_ref[0, :, at], read_ref[1, :, at], here_ref[:, at]
        reads = []
        for h, l, x, (s_high, s_low) in zip(*map(cuts, (high, low, here)), starts):
            reads.append(apply(h, l, stack_pair(s_high)) + mm(h, stack_pair(s_low)) + x)
        spans = [head_sum(x * x, ones) for x in reads]
        mix = beside(*[x * lax.rsqrt(y + 1.0) for x, y in zip(reads, spans)])
        mix = (mix * gain_ref[:, at]).astype(BF16)
        mix_ref[:, at] = mix
        for i, d in enumerate((mine, partner)):
            sums_ref[i] += mm(mix, weights[d, at])

    @pl.when(jnp.logical_not(has_left))
    def _():
        start_buf[...] = jnp.zeros_like(start_buf)

    sums_ref[...] = jnp.zeros_like(sums_ref)
    for load in loads:
        load.wait()

    lag = jnp.maximum(pair - 1, 0)
    slots = 2 * blocks + max(chain - 2, 0)
    plan = [
        (1, [(0, 0)]),
        (2, [(0, 1), (-1, 0)]),
        (blocks - 1, [(0, 2), (-1, 1)]),
    ]
    early = [(blocks + 1, [(0, 3), (-1, 2)]), (blocks + 2, [(-1, 3)]), (2 * blocks + 1, [(3, 0), (3, 1), (2, 0), (3, 2), (2, 1), (1, 0), (3, 3), (2, 2), (2, 3), (1, 1)])]

    def slot(s, carry):
        def pump(which):
            for at, todo in which:
                @pl.when(s == at)
                def _():
                    for part, c in todo:
                        (lend if part < 0 else functools.partial(forward, part))(c)

        pump(early)

        @pl.when(s < blocks)
        def _():
            make(s)

        @pl.when(((s >= 1) & (s < blocks)) | (s == 2 * blocks - 1))
        def _():
            combine(jnp.minimum(s, blocks) - 1)

        b = s - blocks - lag
        live = (b >= 0) & (b < blocks)

        @pl.when(live & has_left)
        def _():
            advance(b)

        @pl.when((s >= blocks) & (s < 2 * blocks))
        def _():
            prepare(s - blocks)

        @pl.when(s == blocks)
        def _():
            own.wait()
            near.wait_recv()

        @pl.when(live)
        def _():
            read(b)

        pump(plan)
        return carry

    lax.fori_loop(0, slots, slot, 0)
    done = [x for at, todo in plan + early if at < slots for x in todo]
    for c in range(pieces):
        for part in (0, 3, 2, 1):
            if (part, c) not in done:
                forward(part, c)

    def project(d):
        at = pl.ds(pl.multiple_of(d * cols, cols), cols)
        out_ref[:, at] = mm(mix_ref[...], weights[d]).astype(BF16)

    for i, d in enumerate((mine, partner)):
        at = pl.ds(pl.multiple_of(d * cols, cols), cols)
        out_ref[:, at] = sums_ref[i].astype(BF16)
    for j in range(others):
        project(behind_of(j))
    for j in range(others):
        for part in range(4):
            for c in range(pieces):
                passed(j, part, c).wait_recv()
        project(lax.rem(partner + columns - 2 * (j + 1), columns))

    near.wait_send()
    for j in range(others):
        for part in range(4):
            for c in range(pieces):
                passed(j, part, c).wait_send()
        for c in range(pieces):
            aside(j, c).wait_send()
            along(j, c).wait_send()
            far(j, 0, c).wait_send()
            far(j, 1, c).wait_send()

    for b in range(blocks):
        give(b).wait_send()

    @pl.when(has_right)
    def _():
        for b in range(blocks):
            copy(b).wait_send()


def per_device(devices, columns, query_rows, key_rows, value_rows, decay_low, rate_low, decay_up,
               rate_up, decay_base, norm_gain, out_weight):
    q = query_rows[0]
    size, width = q.shape
    depth, cols = out_weight.shape
    wide = PAIR * math.gcd(width // PAIR, WIDE)
    blocks = width // wide
    pieces = 4
    others = columns // 2 - 1
    vmem = pl.BlockSpec(memory_space=pltpu.VMEM)
    dma = lambda *dims: pltpu.SemaphoreType.DMA(dims)
    out = pl.pallas_call(
        functools.partial(fused_kernel, devices, columns, wide, pieces),
        in_specs=[pl.BlockSpec(memory_space=pl.ANY)] * 10,
        out_specs=vmem,
        out_shape=jax.ShapeDtypeStruct((size, columns * cols), BF16),
        scratch_shapes=[
            pltpu.VMEM((size, width), BF16),
            pltpu.VMEM((size, width), BF16),
            pltpu.VMEM((size, width), BF16),
            pltpu.VMEM(decay_low.shape[1:], BF16),
            pltpu.VMEM(rate_low.shape[1:], BF16),
            pltpu.VMEM(decay_up.shape, BF16),
            pltpu.VMEM(rate_up.shape, BF16),
            pltpu.VMEM((1, width), F32),
            pltpu.VMEM((1, width), F32),
            dma(9),
            pltpu.VMEM((2, size, cols), F32),
            pltpu.VMEM((columns, depth, cols), BF16),
            pltpu.VMEM((2 * HEAD, width), F32),
            pltpu.VMEM((size, width), F32),
            pltpu.VMEM((10, size, width), BF16),
            pltpu.VMEM((2, size, width), BF16),
            pltpu.VMEM((size, width), F32),
            pltpu.VMEM((2, HEAD, width), BF16),
            pltpu.VMEM((HEAD, width), F32),
            pltpu.VMEM((2, HEAD, width), BF16),
            pltpu.VMEM((HEAD, width), F32),
            pltpu.VMEM((size, width), BF16),
            pltpu.VMEM((blocks, 2 * HEAD, wide), BF16),
            pltpu.VMEM((blocks, 2 * HEAD, wide), BF16),
            pltpu.VMEM((blocks, HEAD, wide), BF16),
            pltpu.VMEM((blocks, HEAD, wide), BF16),
            pltpu.SemaphoreType.DMA,
            dma(2),
            dma(others, 2, pieces),
            dma(others, 2, pieces),
            dma(others, pieces),
            dma(others, pieces),
            dma(others, pieces),
            dma(others, pieces),
            dma(others, 4, pieces),
            dma(others, 4, pieces),
            dma(blocks),
            dma(blocks),
            dma(blocks),
            dma(blocks),
        ],
        compiler_params=pltpu.CompilerParams(collective_id=0, has_side_effects=True),
        name="fused_mixer",
    )(
        q, key_rows[0], value_rows[0], decay_low[0], rate_low[0], decay_up, rate_up,
        decay_base[None], norm_gain[None], out_weight,
    )
    return out[None]


def solution(mesh):
    in_specs = (
        P("dp", "sp", None),
        P("dp", "sp", None),
        P("dp", "sp", None),
        P("dp", "sp", None),
        P("dp", "sp", None),
        P(),
        P(),
        P(),
        P(),
        P(None, "dp"),
    )
    return jax.shard_map(
        functools.partial(per_device, mesh.shape["sp"], mesh.shape["dp"]),
        mesh=mesh, in_specs=in_specs, out_specs=P("dp", "sp", None), check_vma=False,
    )
```

```python
import functools
import math

import jax
import jax.numpy as jnp
from jax import lax
from jax.experimental import pallas as pl
from jax.experimental.pallas import tpu as pltpu
from jax.sharding import PartitionSpec as P

HEAD = 64
PAIR = 2 * HEAD
WIDE = 4
FINE = 16

F32 = jnp.float32
BF16 = jnp.bfloat16


def mm(left, right):
    return lax.dot_general(left, right, (((1,), (0,)), ((), ())), preferred_element_type=F32)


def mm_nt(left, right):
    return lax.dot_general(left, right, (((1,), (1,)), ((), ())), preferred_element_type=F32)


def mm_tn(left, right):
    return lax.dot_general(left, right, (((0,), (0,)), ((), ())), preferred_element_type=F32)


def split(x):
    high = x.astype(BF16)
    return high, (x - high.astype(F32)).astype(BF16)


def mm_ab(left, right, form=mm):
    return form(left[0], right[0]) + form(left[0], right[1]) + form(left[1], right[0])


def beside(*parts):
    return jnp.concatenate(parts, axis=1)


def below(*parts):
    return jnp.concatenate(parts, axis=0)


def swap(x):
    return pltpu.roll(x, HEAD, 1)


def iota(shape, dim):
    return lax.broadcasted_iota(jnp.int32, shape, dim)


def first_half(shape):
    return iota(shape, len(shape) - 1) < HEAD


def stack_pair(x):
    here = lax.rem(iota(x.shape, 1), PAIR) < HEAD
    zero = jnp.zeros_like(x)
    return jnp.concatenate([jnp.where(here, x, zero), jnp.where(here, zero, x)], axis=0)


def head_ones(scale):
    row = iota((PAIR, PAIR), 0)
    col = iota((PAIR, PAIR), 1)
    return jnp.where(row // HEAD == col // HEAD, F32(scale), F32(0.0)).astype(BF16)


def head_sum(x, ones):
    return mm(beside(*split(x)), below(ones, ones))


def crossed(x, y):
    zero = jnp.zeros_like(x)
    return below(beside(x, zero), beside(zero, y))


def solve(parts, size):
    row = iota((size, size), 0)
    col = iota((size, size), 1)
    whole = [beside(z, y) for z, y in parts]
    block = 1
    while block < size:
        last = 2 * block == size
        pick = (row // (2 * block) == col // (2 * block)) & (row // block != col // block)
        fine = block % 16 != 0
        spans = [(0, size)] if fine else [(r + block, r + 2 * block) for r in range(0, size, 2 * block)]
        found = []
        for x in whole:
            high, low = split(x)
            move = jnp.where(pick, high[:, :size], jnp.zeros_like(high[:, :size]))
            move = move if fine else below(*[move[a:b] for a, b in spans])
            if last:
                x, high, low = x[:, size:], high[:, size:], low[:, size:]
            step = mm(beside(move, move), below(high, low))
            if fine:
                found.append(x - step)
            else:
                rows = []
                for i, (a, b) in enumerate(spans):
                    rows += [x[a - block : a], x[a:b] - step[i * block : (i + 1) * block]]
                found.append(below(*rows))
        whole = found
        block *= 2
    return whole


def gates(squashed, rate_low, decay_up, rate_up, base):
    decay_pre = (base + mm(squashed, decay_up)).astype(BF16).astype(F32)
    rate_pre = mm(rate_low, rate_up).astype(BF16).astype(F32)
    log_decay = -math.exp(-0.5) / (1.0 + jnp.exp(-decay_pre))
    rate = 1.0 / (1.0 + jnp.exp(-rate_pre))
    return log_decay, rate


def pair_grid(left, right):
    return mm_nt(beside(*left), beside(right[0], right[0])) + mm_nt(left[0], right[1])


def chunk_maps(pairs):
    size = pairs[0][0].shape[0]
    middle = size // 2
    row = iota((size, size), 0)
    col = iota((size, size), 1)
    strict = row > col
    upto = jnp.where(row >= col, F32(1.0), F32(0.0)).astype(BF16)
    upto = beside(upto, upto)
    ones = head_ones(1.0)
    half = first_half((size, PAIR))
    runs = [mm(upto, below(*split(p[2]))) for p in pairs]
    means = head_ones(1.0 / HEAD)
    sums = []
    values = []
    for p in pairs:
        k = p[0].astype(F32)
        sums.append(head_sum(k * k, ones))
        values.append(split(p[1].astype(F32) - mm(p[1], means)))
    made = []
    for (k, v, log_decay, rate), running, total in zip(pairs, runs, sums):
        k = k.astype(F32)
        centre = running[middle : middle + 1]
        behind = jnp.exp(centre - running)
        unit = k * lax.rsqrt(1.0 + total)
        erase_from = unit * jnp.exp(running - log_decay - centre)
        made.append((erase_from, k * behind, unit * rate * behind, centre, running[size - 1 :]))
    grids = []
    keeps = []
    for erase_from, key_to, erase_to, _, _ in made:
        keeps.append(split(key_to) + split(erase_to))
        key_high, key_low, erase_high, erase_low = keeps[-1]
        right = below(key_high, erase_high), below(key_low, erase_low)
        grids.append(pair_grid(split(stack_pair(erase_from)), right))

    def part(grid, i, j):
        return jnp.where(
            strict, grid[i * size : (i + 1) * size, j * size : (j + 1) * size], 0.0
        )

    parts = []
    for v, grid, (erase_from, _, _, centre, _) in zip(values, grids, made):
        keys = split(beside(part(grid, 0, 0), part(grid, 1, 0)))
        carried = mm_ab(keys, [stack_pair(x) for x in v])
        erase = erase_from * jnp.exp(centre)
        parts.append((part(grid, 0, 1), jnp.where(half, erase, swap(carried))))
        parts.append((part(grid, 1, 1), jnp.where(half, swap(erase), carried)))
    solved = solve(parts, size)
    row2 = iota((PAIR, PAIR), 0)
    col2 = iota((PAIR, PAIR), 1)
    half2 = first_half((HEAD, PAIR))
    fold = lambda x: jnp.where(half2, x[:HEAD], x[HEAD:])
    out = []
    for i, (v, keep, running, (_, key_to, erase_to, centre, final)) in enumerate(
        zip(values, keeps, runs, made)
    ):
        a, b = solved[2 * i], solved[2 * i + 1]
        both = split(beside(jnp.where(half, a, swap(b)), jnp.where(half, swap(a), b)))
        at_end = jnp.exp(final - centre)
        erase_end = split(erase_to * at_end)
        key_end = split(key_to * at_end)
        moved = mm_tn(below(*erase_end), below(both[0], both[0])) + mm_tn(erase_end[0], both[1])
        gained = mm_tn(below(*key_end), below(v[0], v[0])) + mm_tn(key_end[0], v[1])
        decay = jnp.broadcast_to(jnp.exp(final), (PAIR, PAIR))
        transfer = jnp.where(row2 == col2, decay, 0.0) - moved[:, :PAIR]
        added = gained - moved[:, PAIR:]
        halves = tuple(x[:, j : j + PAIR] for j in (0, PAIR) for x in both)
        out.append((fold(transfer), fold(added), running) + keep + halves + v)
    return out


def chunk_reads(pairs):
    size = pairs[0][0].shape[0]
    within = iota((size, size), 0) >= iota((size, size), 1)
    grids = []
    fronts = []
    for q, running, keep in pairs:
        centre = running[size // 2 : size // 2 + 1]
        read_from = q.astype(F32) * jnp.exp(running - centre)
        fronts.append(read_from * jnp.exp(centre))
        right = below(keep[0], keep[2]), below(keep[1], keep[3])
        grids.append(pair_grid(split(stack_pair(read_from)), right))
    out = []
    for (_, _, keep), grid, front in zip(pairs, grids, fronts):
        part = lambda i, j: jnp.where(
            within, grid[i * size : (i + 1) * size, j * size : (j + 1) * size], 0.0
        )
        read_keys = split(beside(part(0, 0), part(1, 0)))
        read_erase = split(beside(part(0, 1), part(1, 1)))
        here = mm_ab(read_keys, [stack_pair(x) for x in keep[8:]])
        both = [stack_pair(beside(keep[i + 4], keep[i + 6])) for i in (0, 1)]
        taken = mm_ab(read_erase, both)
        out.append(split(front - taken[:, :PAIR]) + (here - taken[:, PAIR:],))
    return out


def fused_kernel(devices, columns, wide, pieces, q_hbm, k_hbm, v_hbm, low_hbm, rate_hbm,
                 dup_hbm, rup_hbm, base_hbm, gain_hbm, weight_ref, out_ref, q_ref, k_ref, v_ref,
                 low_ref, rate_ref, dup_ref, rup_ref, base_ref, gain_ref, in_sem, sums_ref, weights,
                 own_ref,
                 running_ref, kept_ref, read_ref, here_ref, first_ref, first_add, both_ref, both_add,
                 mix_ref, give_buf, take_buf, start_buf, end_buf, own_sem, near_sem, far_send,
                 far_recv, side_send, side_recv, long_send, long_recv, pass_send, pass_recv,
                 give_send, give_recv, send_sem, recv_sem):
    me = lax.axis_index("sp")
    mine = lax.axis_index("dp")
    partner = mine + 1 - 2 * lax.rem(mine, 2)
    odd = lax.rem(me, 2)
    pair = me // 2
    side = me + 1 - 2 * odd
    long = me + 2 - 4 * lax.rem(pair, 2)
    width = q_ref.shape[1]
    blocks = width // wide
    chain = devices // 2
    others = columns // 2 - 1
    cols = weight_ref.shape[1]
    piece = weight_ref.shape[0] // (4 * pieces)
    has_left = pair > 0
    has_right = pair < chain - 1
    barrier = pltpu.get_barrier_semaphore()

    def greet(where):
        pl.semaphore_signal(barrier, inc=1, device_id=where, device_id_type=pl.DeviceIdType.MESH)

    def ahead_of(j):
        return lax.rem(mine + 2 * (j + 1), columns)

    def behind_of(j):
        return lax.rem(mine + columns - 2 * (j + 1), columns)

    def remote(src, dst, send, recv, where):
        return pltpu.make_async_remote_copy(
            src_ref=src, dst_ref=dst, send_sem=send, recv_sem=recv,
            device_id=where, device_id_type=pl.DeviceIdType.MESH,
        )

    greet({"dp": partner})
    greet({"sp": side})
    for j in range(others):
        greet({"dp": ahead_of(j)})

    @pl.when(has_left)
    def _():
        greet({"sp": me - 2})

    @pl.when(has_right)
    def _():
        greet({"sp": me + 2})

    inputs = [
        (low_hbm, low_ref), (rate_hbm, rate_ref), (base_hbm, base_ref), (dup_hbm, dup_ref),
        (rup_hbm, rup_ref), (k_hbm, k_ref), (v_hbm, v_ref), (q_hbm, q_ref), (gain_hbm, gain_ref),
    ]
    loads = [pltpu.make_async_copy(x, y, in_sem.at[i]) for i, (x, y) in enumerate(inputs)]
    for load in loads:
        load.start()
    own = pltpu.make_async_copy(weight_ref, weights.at[mine], own_sem)
    own.start()
    pl.semaphore_wait(
        barrier, 2 + others + jnp.minimum(pair, 1) + jnp.minimum(chain - 1 - pair, 1)
    )

    quarter = lax.rem(me, 4)
    side_quarter = quarter + 1 - 2 * odd
    long_quarter = lax.rem(quarter + 2, 4)
    last_quarter = 3 - quarter
    arrivals = (quarter, last_quarter, side_quarter, long_quarter)

    def rows(part, c):
        return pl.ds((part * pieces + c) * piece, piece)

    def far(j, part, c):
        at = rows(arrivals[part], c)
        return remote(
            weight_ref.at[at], weights.at[mine, at],
            far_send.at[j, part, c], far_recv.at[j, part, c], {"dp": ahead_of(j)},
        )

    def spread(j, c, send, recv, where):
        at = rows(quarter, c)
        spot = weights.at[behind_of(j), at]
        return remote(spot, spot, send.at[j, c], recv.at[j, c], {"sp": where})

    def aside(j, c):
        return spread(j, c, side_send, side_recv, side)

    def along(j, c):
        return spread(j, c, long_send, long_recv, long)

    def passed(j, part, c):
        spot = weights.at[behind_of(j), rows(arrivals[part], c)]
        return remote(
            spot, spot, pass_send.at[j, part, c], pass_recv.at[j, part, c], {"dp": partner},
        )

    near = remote(weight_ref, weights.at[mine], near_sem.at[0], near_sem.at[1], {"dp": partner})
    for part in range(2):
        for c in range(pieces):
            for j in range(others):
                far(j, part, c).start()
    near.start()

    def forward(part, c):
        for j in range(others):
            if part < 2:
                far(j, part, c).wait_recv()
            elif part == 2:
                aside(j, c).wait_recv()
            else:
                along(j, c).wait_recv()
            if part == 0:
                along(j, c).start()
            passed(j, part, c).start()

    def lend(c):
        for j in range(others):
            aside(j, c).start()

    def lanes_of(g):
        return pl.ds(pl.multiple_of(g * wide, wide), wide)

    def cut(x, i):
        return x[:, i * PAIR : (i + 1) * PAIR]

    def cuts(x):
        return [cut(x, i) for i in range(wide // PAIR)]

    def give(b):
        return remote(
            give_buf.at[b], take_buf.at[b], give_send.at[b], give_recv.at[b], {"sp": side}
        )

    def copy(b, i):
        return remote(
            end_buf.at[b, i], start_buf.at[b, i], send_sem.at[b, i], recv_sem.at[b, i],
            {"sp": lax.rem(me + 2, devices)},
        )

    shares = end_buf.shape[1]
    share = wide // shares

    def start_of(b):
        return beside(*[start_buf[b, i] for i in range(shares)])

    def make(b):
        at = lanes_of(b)
        squashed = jnp.tanh(low_ref[...].astype(F32)).astype(BF16)
        log_decay, rate = gates(
            squashed, rate_ref[...], dup_ref[:, at], rup_ref[:, at], base_ref[:, at]
        )
        pairs = list(zip(*map(cuts, (k_ref[:, at], v_ref[:, at], log_decay, rate))))
        parts = [beside(*part) for part in zip(*chunk_maps(pairs))]
        maps = below(parts[0], parts[1])
        own_ref[:, at] = maps
        give_buf[b] = maps.astype(BF16)
        running_ref[:, at] = parts[2]
        for i, part in enumerate(parts[3:]):
            kept_ref[i, :, at] = part
        give(b).start()

    def combine(b):
        at = lanes_of(b)
        give(b).wait_recv()
        own, taken = own_ref[:, at], take_buf[b].astype(F32)
        is_odd = iota(own.shape, 0) * 0 + odd == 1
        first, second = jnp.where(is_odd, taken, own), jnp.where(is_odd, own, taken)
        found = []
        for x, y in zip(cuts(first), cuts(second)):
            left = split(y[:HEAD])
            right = split(beside(stack_pair(x[:HEAD]), stack_pair(x[HEAD:])))
            found.append((mm_ab(left, right), y[HEAD:]))
        both = beside(*[x[:, :PAIR] for x, _ in found])
        added = beside(*[x[:, PAIR:] + y for x, y in found])
        both_ref[0, :, at], both_ref[1, :, at] = split(both)
        both_add[:, at] = added
        same = (iota((HEAD, wide), 1) % HEAD == iota((HEAD, wide), 0)).astype(F32)
        is_odd = is_odd[:HEAD]
        first_ref[0, :, at], first_ref[1, :, at] = split(jnp.where(is_odd, first[:HEAD], same))
        first_add[:, at] = jnp.where(is_odd, first[HEAD:], 0.0)

        @pl.when(jnp.logical_not(has_left) & has_right)
        def _():
            for i in range(shares):
                end_buf[b, i] = added[:, i * share : (i + 1) * share].astype(BF16)
                copy(b, i).start()

    def apply(high, low, state):
        return mm(beside(high, low), below(state, state))

    def advance(b):
        for i in range(shares):
            copy(b, i).wait_recv()

            @pl.when(has_right)
            def _():
                at = pl.ds(pl.multiple_of(b * wide + i * share, share), share)
                high, low, start = both_ref[0, :, at], both_ref[1, :, at], start_buf[b, i]
                ends = []
                for j in range(share // PAIR):
                    h, l, x = cut(high, j), cut(low, j), cut(start, j)
                    ends.append(apply(h, l, stack_pair(x)))
                end_buf[b, i] = (beside(*ends) + both_add[:, at]).astype(BF16)
                copy(b, i).start()

    def prepare(b):
        at = lanes_of(b)
        kept = [cuts(kept_ref[j, :, at]) for j in range(kept_ref.shape[0])]
        keeps = list(zip(*kept))
        pairs = list(zip(*map(cuts, (q_ref[:, at], running_ref[:, at])), keeps))
        high, low, here = [beside(*part) for part in zip(*chunk_reads(pairs))]
        read_ref[0, :, at], read_ref[1, :, at], here_ref[:, at] = high, low, here

    ones = head_ones(1.0 / HEAD)

    def read(b):
        at = lanes_of(b)
        high, low, start = first_ref[0, :, at], first_ref[1, :, at], start_of(b)
        starts = [apply(h, l, stack_pair(x)) for h, l, x in zip(*map(cuts, (high, low, start)))]
        starts = [split(x + y) for x, y in zip(starts, cuts(first_add[:, at]))]
        high, low, here = read_ref[0, :, at], read_ref[1, :, at], here_ref[:, at]
        reads = []
        for h, l, x, (s_high, s_low) in zip(*map(cuts, (high, low, here)), starts):
            reads.append(apply(h, l, stack_pair(s_high)) + mm(h, stack_pair(s_low)) + x)
        spans = [head_sum(x * x, ones) for x in reads]
        mix = beside(*[x * lax.rsqrt(y + 1.0) for x, y in zip(reads, spans)])
        mix = (mix * gain_ref[:, at]).astype(BF16)
        mix_ref[:, at] = mix
        for i, d in enumerate((mine, partner)):
            sums_ref[i] += mm(mix, weights[d, at])

    @pl.when(jnp.logical_not(has_left))
    def _():
        start_buf[...] = jnp.zeros_like(start_buf)

    sums_ref[...] = jnp.zeros_like(sums_ref)
    for load in loads:
        load.wait()

    lag = jnp.maximum(pair - 1, 0)
    slots = 2 * blocks + max(chain - 2, 0)
    plan = [
        (1, [(0, 0)]),
        (2, [(0, 1), (-1, 0)]),
        (blocks - 1, [(0, 2), (-1, 1)]),
    ]
    early = [(blocks + 1, [(0, 3), (-1, 2)]), (blocks + 2, [(-1, 3)]), (2 * blocks, [(3, 0), (3, 1), (2, 0), (3, 2), (2, 1), (1, 0)]), (2 * blocks + 1, [(3, 3), (2, 2), (2, 3), (1, 1)])]

    def slot(s, carry):
        def pump(which):
            for at, todo in which:
                @pl.when(s == at)
                def _():
                    for part, c in todo:
                        (lend if part < 0 else functools.partial(forward, part))(c)

        pump(early)

        @pl.when(s < blocks)
        def _():
            make(s)

        @pl.when(((s >= 1) & (s < blocks)) | (s == 2 * blocks - 1))
        def _():
            combine(jnp.minimum(s, blocks) - 1)

        b = s - blocks - lag
        live = (b >= 0) & (b < blocks)

        @pl.when(live & has_left)
        def _():
            advance(b)

        @pl.when((s >= blocks) & (s < 2 * blocks))
        def _():
            prepare(s - blocks)

        @pl.when(s == blocks)
        def _():
            own.wait()
            near.wait_recv()

        @pl.when(live)
        def _():
            read(b)

        pump(plan)
        return carry

    lax.fori_loop(0, slots, slot, 0)
    done = [x for at, todo in plan + early if at < slots for x in todo]
    for c in range(pieces):
        for part in (0, 3, 2, 1):
            if (part, c) not in done:
                forward(part, c)

    def project(d):
        at = pl.ds(pl.multiple_of(d * cols, cols), cols)
        out_ref[:, at] = mm(mix_ref[...], weights[d]).astype(BF16)

    for i, d in enumerate((mine, partner)):
        at = pl.ds(pl.multiple_of(d * cols, cols), cols)
        out_ref[:, at] = sums_ref[i].astype(BF16)
    for j in range(others):
        project(behind_of(j))
    for j in range(others):
        for part in range(4):
            for c in range(pieces):
                passed(j, part, c).wait_recv()
        project(lax.rem(partner + columns - 2 * (j + 1), columns))

    near.wait_send()
    for j in range(others):
        for part in range(4):
            for c in range(pieces):
                passed(j, part, c).wait_send()
        for c in range(pieces):
            aside(j, c).wait_send()
            along(j, c).wait_send()
            far(j, 0, c).wait_send()
            far(j, 1, c).wait_send()

    for b in range(blocks):
        give(b).wait_send()

    @pl.when(has_right)
    def _():
        for b in range(blocks):
            for i in range(shares):
                copy(b, i).wait_send()


def pin(x):
    return pltpu.with_memory_space_constraint(x, pltpu.HBM)


def per_device(devices, columns, query_rows, key_rows, value_rows, decay_low, rate_low, decay_up,
               rate_up, decay_base, norm_gain, out_weight):
    q = query_rows[0]
    size, width = q.shape
    depth, cols = out_weight.shape
    wide = PAIR * math.gcd(width // PAIR, WIDE)
    blocks = width // wide
    shares = math.gcd(wide // PAIR, 2)
    pieces = 4
    others = columns // 2 - 1
    vmem = pl.BlockSpec(memory_space=pltpu.VMEM)
    dma = lambda *dims: pltpu.SemaphoreType.DMA(dims)
    out = pl.pallas_call(
        functools.partial(fused_kernel, devices, columns, wide, pieces),
        in_specs=[pl.BlockSpec(memory_space=pl.ANY)] * 10,
        out_specs=vmem,
        out_shape=jax.ShapeDtypeStruct((size, columns * cols), BF16),
        scratch_shapes=[
            pltpu.VMEM((size, width), BF16),
            pltpu.VMEM((size, width), BF16),
            pltpu.VMEM((size, width), BF16),
            pltpu.VMEM(decay_low.shape[1:], BF16),
            pltpu.VMEM(rate_low.shape[1:], BF16),
            pltpu.VMEM(decay_up.shape, BF16),
            pltpu.VMEM(rate_up.shape, BF16),
            pltpu.VMEM((1, width), F32),
            pltpu.VMEM((1, width), F32),
            dma(9),
            pltpu.VMEM((2, size, cols), F32),
            pltpu.VMEM((columns, depth, cols), BF16),
            pltpu.VMEM((2 * HEAD, width), F32),
            pltpu.VMEM((size, width), F32),
            pltpu.VMEM((10, size, width), BF16),
            pltpu.VMEM((2, size, width), BF16),
            pltpu.VMEM((size, width), F32),
            pltpu.VMEM((2, HEAD, width), BF16),
            pltpu.VMEM((HEAD, width), F32),
            pltpu.VMEM((2, HEAD, width), BF16),
            pltpu.VMEM((HEAD, width), F32),
            pltpu.VMEM((size, width), BF16),
            pltpu.VMEM((blocks, 2 * HEAD, wide), BF16),
            pltpu.VMEM((blocks, 2 * HEAD, wide), BF16),
            pltpu.VMEM((blocks, shares, HEAD, wide // shares), BF16),
            pltpu.VMEM((blocks, shares, HEAD, wide // shares), BF16),
            pltpu.SemaphoreType.DMA,
            dma(2),
            dma(others, 2, pieces),
            dma(others, 2, pieces),
            dma(others, pieces),
            dma(others, pieces),
            dma(others, pieces),
            dma(others, pieces),
            dma(others, 4, pieces),
            dma(others, 4, pieces),
            dma(blocks),
            dma(blocks),
            dma(blocks, shares),
            dma(blocks, shares),
        ],
        compiler_params=pltpu.CompilerParams(collective_id=0, has_side_effects=True, vmem_limit_bytes=45 * 2**20),
        name="fused_mixer",
    )(
        *map(pin, (q, key_rows[0], value_rows[0], decay_low[0], rate_low[0], decay_up, rate_up,
        decay_base[None], norm_gain[None], out_weight)),
    )
    return out[None]


def solution(mesh):
    in_specs = (
        P("dp", "sp", None),
        P("dp", "sp", None),
        P("dp", "sp", None),
        P("dp", "sp", None),
        P("dp", "sp", None),
        P(),
        P(),
        P(),
        P(),
        P(None, "dp"),
    )
    return jax.shard_map(
        functools.partial(per_device, mesh.shape["sp"], mesh.shape["dp"]),
        mesh=mesh, in_specs=in_specs, out_specs=P("dp", "sp", None), check_vma=False,
    )
```

```python
import functools
import math

import jax
import jax.numpy as jnp
from jax import lax
from jax.experimental import pallas as pl
from jax.experimental.pallas import tpu as pltpu
from jax.sharding import PartitionSpec as P

HEAD = 64
PAIR = 2 * HEAD
WIDE = 4
FINE = 16
FINE = 16

F32 = jnp.float32
BF16 = jnp.bfloat16


def mm(left, right):
    return lax.dot_general(left, right, (((1,), (0,)), ((), ())), preferred_element_type=F32)


def mm_nt(left, right):
    return lax.dot_general(left, right, (((1,), (1,)), ((), ())), preferred_element_type=F32)


def mm_tn(left, right):
    return lax.dot_general(left, right, (((0,), (0,)), ((), ())), preferred_element_type=F32)


def split(x):
    high = x.astype(BF16)
    return high, (x - high.astype(F32)).astype(BF16)


def mm_ab(left, right, form=mm):
    return form(left[0], right[0]) + form(left[0], right[1]) + form(left[1], right[0])


def beside(*parts):
    return jnp.concatenate(parts, axis=1)


def below(*parts):
    return jnp.concatenate(parts, axis=0)


def swap(x):
    return pltpu.roll(x, HEAD, 1)


def iota(shape, dim):
    return lax.broadcasted_iota(jnp.int32, shape, dim)


def first_half(shape):
    return iota(shape, len(shape) - 1) < HEAD


def stack_pair(x):
    here = lax.rem(iota(x.shape, 1), PAIR) < HEAD
    zero = jnp.zeros_like(x)
    return jnp.concatenate([jnp.where(here, x, zero), jnp.where(here, zero, x)], axis=0)


def head_ones(scale):
    row = iota((PAIR, PAIR), 0)
    col = iota((PAIR, PAIR), 1)
    return jnp.where(row // HEAD == col // HEAD, F32(scale), F32(0.0)).astype(BF16)


def head_sum(x, ones):
    return mm(beside(*split(x)), below(ones, ones))


def crossed(x, y):
    zero = jnp.zeros_like(x)
    return below(beside(x, zero), beside(zero, y))


def crossed(x, y):
    zero = jnp.zeros_like(x)
    return below(beside(x, zero), beside(zero, y))


def solve(parts, size):
    row = iota((size, size), 0)
    col = iota((size, size), 1)

    def picked(x, block):
        keep = (row // (2 * block) == col // (2 * block)) & (row // block != col // block)
        return jnp.where(keep, x, jnp.zeros_like(x))

    small = [jnp.where(row // FINE == col // FINE, z, 0.0) for z, _ in parts]
    block = 1
    while block < FINE:
        high = [x.astype(BF16) for x in small]
        steps = []
        for x, y in zip(high[::2], high[1::2]):
            both = mm(beside(picked(x, block), picked(y, block)), crossed(x, y))
            steps += [both[:, :size], both[:, size:]]
        small = [x - step for x, step in zip(small, steps)]
        block *= 2
    whole = []
    for (z, y), x in zip(parts, small):
        x = x.astype(BF16)
        both = beside(z, y)
        whole.append(both - mm(beside(x, x), below(*split(both))))
    while block < size:
        keep = (row // (2 * block) == col // (2 * block)) & (row // block != col // block)
        found = []
        for x in whole:
            first = size if 2 * block == size else 0
            moves, high, low, evens, odds = [], [], [], [], []
            for r in range(0, size, 2 * block):
                m, n = r + block, r + 2 * block
                z = x[m:n, :size].astype(BF16)
                moves.append(jnp.where(keep[m:n], z, jnp.zeros_like(z)))
                evens.append(x[r:m, first:])
                odds.append(x[m:n, first:])
                for parts_of, piece in zip((high, low), split(evens[-1])):
                    parts_of += [piece, jnp.zeros_like(piece)]
            move = below(*moves)
            step = mm(beside(move, move), below(*high, *low))
            rows = []
            for i, (even, odd) in enumerate(zip(evens, odds)):
                rows += [even, odd - step[i * block : (i + 1) * block]]
            found.append(below(*rows))
        whole = found
        block *= 2
    return whole


def gates(squashed, rate_low, decay_up, rate_up, base):
    decay_pre = (base + mm(squashed, decay_up)).astype(BF16).astype(F32)
    rate_pre = mm(rate_low, rate_up).astype(BF16).astype(F32)
    log_decay = -math.exp(-0.5) / (1.0 + jnp.exp(-decay_pre))
    rate = 1.0 / (1.0 + jnp.exp(-rate_pre))
    return log_decay, rate


def pair_grid(left, right):
    return mm_nt(beside(*left), beside(right[0], right[0])) + mm_nt(left[0], right[1])


def chunk_maps(pairs):
    size = pairs[0][0].shape[0]
    middle = size // 2
    row = iota((size, size), 0)
    col = iota((size, size), 1)
    strict = row > col
    upto = jnp.where(row >= col, F32(1.0), F32(0.0)).astype(BF16)
    upto = beside(upto, upto)
    ones = head_ones(1.0)
    half = first_half((size, PAIR))
    runs = [mm(upto, below(*split(p[2]))) for p in pairs]
    means = head_ones(1.0 / HEAD)
    sums = []
    values = []
    for p in pairs:
        k = p[0].astype(F32)
        sums.append(mm((k * k).astype(BF16), ones))
        values.append(split(p[1].astype(F32) - mm(p[1], means)))
    made = []
    for (k, v, log_decay, rate), running, total in zip(pairs, runs, sums):
        k = k.astype(F32)
        centre = running[middle : middle + 1]
        behind = jnp.exp(centre - running)
        unit = k * lax.rsqrt(1.0 + total)
        erase_from = unit * jnp.exp(running - log_decay - centre)
        made.append((erase_from, k * behind, unit * rate * behind, centre, running[size - 1 :]))
    grids = []
    keeps = []
    for erase_from, key_to, erase_to, _, _ in made:
        keeps.append(split(key_to) + split(erase_to))
        key_high, key_low, erase_high, erase_low = keeps[-1]
        right = below(key_high, erase_high), below(key_low, erase_low)
        grids.append(pair_grid(split(stack_pair(erase_from)), right))

    def part(grid, i, j):
        return jnp.where(
            strict, grid[i * size : (i + 1) * size, j * size : (j + 1) * size], 0.0
        )

    parts = []
    for v, grid, (erase_from, _, _, centre, _) in zip(values, grids, made):
        keys = split(beside(part(grid, 0, 0), part(grid, 1, 0)))
        carried = mm_ab(keys, [stack_pair(x) for x in v])
        erase = erase_from * jnp.exp(centre)
        parts.append((part(grid, 0, 1), jnp.where(half, erase, swap(carried))))
        parts.append((part(grid, 1, 1), jnp.where(half, swap(erase), carried)))
    solved = solve(parts, size)
    row2 = iota((PAIR, PAIR), 0)
    col2 = iota((PAIR, PAIR), 1)
    half2 = first_half((HEAD, PAIR))
    fold = lambda x: jnp.where(half2, x[:HEAD], x[HEAD:])
    out = []
    for i, (v, keep, running, (_, _, _, centre, final)) in enumerate(
        zip(values, keeps, runs, made)
    ):
        a, b = solved[2 * i], solved[2 * i + 1]
        both = split(beside(jnp.where(half, a, swap(b)), jnp.where(half, swap(a), b)))
        at_end = fold(jnp.transpose(jnp.broadcast_to(jnp.exp(final - centre), (PAIR, PAIR))))
        moved = mm_tn(below(*keep[2:]), below(both[0], both[0])) + mm_tn(keep[2], both[1])
        gained = mm_tn(below(*keep[:2]), below(v[0], v[0])) + mm_tn(keep[0], v[1])
        decay = jnp.where(row2 == col2, jnp.broadcast_to(jnp.exp(final), (PAIR, PAIR)), 0.0)
        transfer = fold(decay) - fold(moved[:, :PAIR]) * at_end
        added = fold(gained - moved[:, PAIR:]) * at_end
        halves = tuple(x[:, j : j + PAIR] for j in (0, PAIR) for x in both)
        out.append((transfer, added, running) + keep + halves + v)
    return out


def chunk_reads(pairs):
    size = pairs[0][0].shape[0]
    within = iota((size, size), 0) >= iota((size, size), 1)
    grids = []
    fronts = []
    for q, running, keep in pairs:
        centre = running[size // 2 : size // 2 + 1]
        read_from = q.astype(F32) * jnp.exp(running - centre)
        fronts.append(read_from * jnp.exp(centre))
        right = below(keep[0], keep[2]), below(keep[1], keep[3])
        grids.append(pair_grid(split(stack_pair(read_from)), right))
    out = []
    for (_, _, keep), grid, front in zip(pairs, grids, fronts):
        part = lambda i, j: jnp.where(
            within, grid[i * size : (i + 1) * size, j * size : (j + 1) * size], 0.0
        )
        read_keys = split(beside(part(0, 0), part(1, 0)))
        read_erase = split(beside(part(0, 1), part(1, 1)))
        here = mm_ab(read_keys, [stack_pair(x) for x in keep[8:]])
        both = [stack_pair(beside(keep[i + 4], keep[i + 6])) for i in (0, 1)]
        taken = mm_ab(read_erase, both)
        out.append(split(front - taken[:, :PAIR]) + (here - taken[:, PAIR:],))
    return out


def fused_kernel(devices, columns, wide, pieces, q_hbm, k_hbm, v_hbm, low_hbm, rate_hbm,
                 dup_hbm, rup_hbm, base_hbm, gain_hbm, weight_ref, out_ref, q_ref, k_ref, v_ref,
                 low_ref, rate_ref, dup_ref, rup_ref, base_ref, gain_ref, in_sem, sums_ref, weights,
                 own_ref,
                 running_ref, kept_ref, read_ref, here_ref, first_ref, first_add, both_ref, both_add,
                 mix_ref, give_buf, take_buf, start_buf, end_buf, own_sem, near_sem, far_send,
                 far_recv, side_send, side_recv, long_send, long_recv, pass_send, pass_recv,
                 give_send, give_recv, send_sem, recv_sem):
    me = lax.axis_index("sp")
    mine = lax.axis_index("dp")
    partner = mine + 1 - 2 * lax.rem(mine, 2)
    odd = lax.rem(me, 2)
    pair = me // 2
    side = me + 1 - 2 * odd
    long = me + 2 - 4 * lax.rem(pair, 2)
    width = q_ref.shape[1]
    blocks = width // wide
    chain = devices // 2
    others = columns // 2 - 1
    cols = weight_ref.shape[1]
    piece = weight_ref.shape[0] // (4 * pieces)
    has_left = pair > 0
    has_right = pair < chain - 1
    barrier = pltpu.get_barrier_semaphore()

    def greet(where):
        pl.semaphore_signal(barrier, inc=1, device_id=where, device_id_type=pl.DeviceIdType.MESH)

    def ahead_of(j):
        return lax.rem(mine + 2 * (j + 1), columns)

    def behind_of(j):
        return lax.rem(mine + columns - 2 * (j + 1), columns)

    def remote(src, dst, send, recv, where):
        return pltpu.make_async_remote_copy(
            src_ref=src, dst_ref=dst, send_sem=send, recv_sem=recv,
            device_id=where, device_id_type=pl.DeviceIdType.MESH,
        )

    inputs = [
        (low_hbm, low_ref), (rate_hbm, rate_ref), (base_hbm, base_ref), (dup_hbm, dup_ref),
        (rup_hbm, rup_ref), (k_hbm, k_ref), (v_hbm, v_ref), (q_hbm, q_ref), (gain_hbm, gain_ref),
    ]
    loads = [pltpu.make_async_copy(x, y, in_sem.at[i]) for i, (x, y) in enumerate(inputs)]
    for load in loads:
        load.start()
    greet({"dp": partner})
    greet({"sp": side})
    for j in range(others):
        greet({"dp": ahead_of(j)})

    @pl.when(has_left)
    def _():
        greet({"sp": me - 2})

    @pl.when(has_right)
    def _():
        greet({"sp": me + 2})

    own = pltpu.make_async_copy(weight_ref, weights.at[mine], own_sem)
    pl.semaphore_wait(
        barrier, 2 + others + jnp.minimum(pair, 1) + jnp.minimum(chain - 1 - pair, 1)
    )

    quarter = lax.rem(me, 4)
    side_quarter = quarter + 1 - 2 * odd
    long_quarter = lax.rem(quarter + 2, 4)
    last_quarter = 3 - quarter
    arrivals = (quarter, last_quarter, side_quarter, long_quarter)

    def rows(part, c):
        return pl.ds((part * pieces + c) * piece, piece)

    def far(j, part, c):
        at = rows(arrivals[part], c)
        return remote(
            weight_ref.at[at], weights.at[mine, at],
            far_send.at[j, part, c], far_recv.at[j, part, c], {"dp": ahead_of(j)},
        )

    def spread(j, c, send, recv, where):
        at = rows(quarter, c)
        spot = weights.at[behind_of(j), at]
        return remote(spot, spot, send.at[j, c], recv.at[j, c], {"sp": where})

    def aside(j, c):
        return spread(j, c, side_send, side_recv, side)

    def along(j, c):
        return spread(j, c, long_send, long_recv, long)

    def passed(j, part, c):
        spot = weights.at[behind_of(j), rows(arrivals[part], c)]
        return remote(
            spot, spot, pass_send.at[j, part, c], pass_recv.at[j, part, c], {"dp": partner},
        )

    near = remote(weight_ref, weights.at[mine], near_sem.at[0], near_sem.at[1], {"dp": partner})
    for part in range(2):
        for c in range(pieces):
            for j in range(others):
                far(j, part, c).start()

    def forward(part, c):
        for j in range(others):
            if part < 2:
                far(j, part, c).wait_recv()
            elif part == 2:
                aside(j, c).wait_recv()
            else:
                along(j, c).wait_recv()
            if part == 0:
                along(j, c).start()
            passed(j, part, c).start()

    def lend(c):
        for j in range(others):
            aside(j, c).start()

    def lanes_of(g):
        return pl.ds(pl.multiple_of(g * wide, wide), wide)

    def cut(x, i):
        return x[:, i * PAIR : (i + 1) * PAIR]

    def cuts(x):
        return [cut(x, i) for i in range(wide // PAIR)]

    def give(b):
        return remote(
            give_buf.at[b], take_buf.at[b], give_send.at[b], give_recv.at[b], {"sp": side}
        )

    def copy(b, i):
        return remote(
            end_buf.at[b, i], start_buf.at[b, i], send_sem.at[b, i], recv_sem.at[b, i],
            {"sp": lax.rem(me + 2, devices)},
        )

    shares = end_buf.shape[1]
    share = wide // shares

    def start_of(b):
        return beside(*[start_buf[b, i] for i in range(shares)])

    def make(b):
        at = lanes_of(b)
        squashed = jnp.tanh(low_ref[...].astype(F32)).astype(BF16)
        log_decay, rate = gates(
            squashed, rate_ref[...], dup_ref[:, at], rup_ref[:, at], base_ref[:, at]
        )
        pairs = list(zip(*map(cuts, (k_ref[:, at], v_ref[:, at], log_decay, rate))))
        parts = [beside(*part) for part in zip(*chunk_maps(pairs))]
        maps = below(parts[0], parts[1])
        own_ref[:, at] = maps
        give_buf[b] = maps.astype(BF16)
        running_ref[:, at] = parts[2]
        for i, part in enumerate(parts[3:]):
            kept_ref[i, :, at] = part
        give(b).start()

    def combine(b):
        at = lanes_of(b)
        give(b).wait_recv()
        own, taken = own_ref[:, at], take_buf[b].astype(F32)
        is_odd = iota(own.shape, 0) * 0 + odd == 1
        first, second = jnp.where(is_odd, taken, own), jnp.where(is_odd, own, taken)
        found = []
        for x, y in zip(cuts(first), cuts(second)):
            left = split(y[:HEAD])
            right = split(beside(stack_pair(x[:HEAD]), stack_pair(x[HEAD:])))
            found.append((mm_ab(left, right), y[HEAD:]))
        both = beside(*[x[:, :PAIR] for x, _ in found])
        added = beside(*[x[:, PAIR:] + y for x, y in found])
        both_ref[0, :, at], both_ref[1, :, at] = split(both)
        both_add[:, at] = added
        same = (iota((HEAD, wide), 1) % HEAD == iota((HEAD, wide), 0)).astype(F32)
        is_odd = is_odd[:HEAD]
        first_ref[0, :, at], first_ref[1, :, at] = split(jnp.where(is_odd, first[:HEAD], same))
        first_add[:, at] = jnp.where(is_odd, first[HEAD:], 0.0)

        @pl.when(jnp.logical_not(has_left) & has_right)
        def _():
            for i in range(shares):
                end_buf[b, i] = added[:, i * share : (i + 1) * share].astype(BF16)
                copy(b, i).start()

    def apply(high, low, state):
        return mm(beside(high, low), below(state, state))

    def advance(b):
        for i in range(shares):
            copy(b, i).wait_recv()

            @pl.when(has_right)
            def _():
                at = pl.ds(pl.multiple_of(b * wide + i * share, share), share)
                high, low, start = both_ref[0, :, at], both_ref[1, :, at], start_buf[b, i]
                ends = []
                for j in range(share // PAIR):
                    h, l, x = cut(high, j), cut(low, j), cut(start, j)
                    ends.append(apply(h, l, stack_pair(x)))
                end_buf[b, i] = (beside(*ends) + both_add[:, at]).astype(BF16)
                copy(b, i).start()

    def prepare(b):
        at = lanes_of(b)
        kept = [cuts(kept_ref[j, :, at]) for j in range(kept_ref.shape[0])]
        keeps = list(zip(*kept))
        pairs = list(zip(*map(cuts, (q_ref[:, at], running_ref[:, at])), keeps))
        high, low, here = [beside(*part) for part in zip(*chunk_reads(pairs))]
        read_ref[0, :, at], read_ref[1, :, at], here_ref[:, at] = high, low, here

    ones = head_ones(1.0 / HEAD)

    def read(b):
        at = lanes_of(b)
        high, low, start = first_ref[0, :, at], first_ref[1, :, at], start_of(b)
        starts = [apply(h, l, stack_pair(x)) for h, l, x in zip(*map(cuts, (high, low, start)))]
        starts = [split(x + y) for x, y in zip(starts, cuts(first_add[:, at]))]
        high, low, here = read_ref[0, :, at], read_ref[1, :, at], here_ref[:, at]
        reads = []
        for h, l, x, (s_high, s_low) in zip(*map(cuts, (high, low, here)), starts):
            reads.append(apply(h, l, stack_pair(s_high)) + mm(h, stack_pair(s_low)) + x)
        spans = [head_sum(x * x, ones) for x in reads]
        mix = beside(*[x * lax.rsqrt(y + 1.0) for x, y in zip(reads, spans)])
        mix = (mix * gain_ref[:, at]).astype(BF16)
        mix_ref[:, at] = mix
        for i, d in enumerate((mine, partner)):
            sums_ref[i] += mm(mix, weights[d, at])

    @pl.when(jnp.logical_not(has_left))
    def _():
        start_buf[...] = jnp.zeros_like(start_buf)

    sums_ref[:2] = jnp.zeros((2, *sums_ref.shape[1:]), F32)
    for load in loads:
        load.wait()
    own.start()
    near.start()

    lag = jnp.maximum(pair - 1, 0)
    slots = 2 * blocks + max(chain - 2, 0)
    plan = [
        (1, [(0, 0)]),
        (2, [(0, 1), (-1, 0)]),
        (blocks - 1, [(0, 2), (-1, 1)]),
    ]
    early = [
        (blocks + 1, [(0, 3), (-1, 2)]),
        (blocks + 2, [(-1, 3)]),
        (2 * blocks, [(3, 0), (3, 1), (2, 0), (3, 2), (2, 1), (1, 0)]),
    ]
    done = [x for at, todo in plan + early if at < slots - 1 for x in todo]
    head = (blocks - 1) * wide
    far_columns = [
        d for j in range(others)
        for d in (behind_of(j), lax.rem(partner + columns - 2 * (j + 1), columns))
    ]

    def slot(s, carry):
        def pump(which):
            for at, todo in [x for x in which if x[0] < slots - 1]:
                @pl.when(s == at)
                def _():
                    for part, c in todo:
                        (lend if part < 0 else functools.partial(forward, part))(c)

        pump(early)

        @pl.when(s == slots - 1)
        def _():
            for c in range(pieces):
                for part in (3, 2, 1, 0):
                    if (part, c) not in done:
                        forward(part, c)
            for j in range(others):
                for part in range(4):
                    for c in range(pieces):
                        passed(j, part, c).wait_recv()
            for i, d in enumerate(far_columns):
                sums_ref[2 + i] = mm(mix_ref[:, :head], weights[d, :head])

        @pl.when(s < blocks)
        def _():
            make(s)

        @pl.when(((s >= 1) & (s < blocks)) | (s == 2 * blocks - 1))
        def _():
            combine(jnp.minimum(s, blocks) - 1)

        b = s - blocks - lag
        live = (b >= 0) & (b < blocks)

        @pl.when(live & has_left)
        def _():
            advance(b)

        @pl.when((s >= blocks) & (s < 2 * blocks))
        def _():
            prepare(s - blocks)

        @pl.when(s == blocks)
        def _():
            own.wait()
            near.wait_recv()

        @pl.when(live)
        def _():
            read(b)

        pump(plan)
        return carry

    lax.fori_loop(0, slots, slot, 0)
    def columns_of(d):
        return pl.ds(pl.multiple_of(d * cols, cols), cols)

    for i, d in enumerate((mine, partner)):
        out_ref[:, columns_of(d)] = sums_ref[i].astype(BF16)
    for i, d in enumerate(far_columns):
        rest = mm(mix_ref[:, head:], weights[d, head:])
        out_ref[:, columns_of(d)] = (sums_ref[2 + i] + rest).astype(BF16)

    near.wait_send()
    for j in range(others):
        for part in range(4):
            for c in range(pieces):
                passed(j, part, c).wait_send()
        for c in range(pieces):
            aside(j, c).wait_send()
            along(j, c).wait_send()
            far(j, 0, c).wait_send()
            far(j, 1, c).wait_send()

    for b in range(blocks):
        give(b).wait_send()

    @pl.when(has_right)
    def _():
        for b in range(blocks):
            for i in range(shares):
                copy(b, i).wait_send()


def pin(x):
    return pltpu.with_memory_space_constraint(x, pltpu.HBM)


def per_device(devices, columns, query_rows, key_rows, value_rows, decay_low, rate_low, decay_up,
               rate_up, decay_base, norm_gain, out_weight):
    q = query_rows[0]
    size, width = q.shape
    depth, cols = out_weight.shape
    wide = PAIR * math.gcd(width // PAIR, WIDE)
    blocks = width // wide
    shares = math.gcd(wide // PAIR, 2)
    pieces = 4
    others = columns // 2 - 1
    vmem = pl.BlockSpec(memory_space=pltpu.VMEM)
    dma = lambda *dims: pltpu.SemaphoreType.DMA(dims)
    out = pl.pallas_call(
        functools.partial(fused_kernel, devices, columns, wide, pieces),
        in_specs=[pl.BlockSpec(memory_space=pl.ANY)] * 10,
        out_specs=vmem,
        out_shape=jax.ShapeDtypeStruct((size, columns * cols), BF16),
        scratch_shapes=[
            pltpu.VMEM((size, width), BF16),
            pltpu.VMEM((size, width), BF16),
            pltpu.VMEM((size, width), BF16),
            pltpu.VMEM(decay_low.shape[1:], BF16),
            pltpu.VMEM(rate_low.shape[1:], BF16),
            pltpu.VMEM(decay_up.shape, BF16),
            pltpu.VMEM(rate_up.shape, BF16),
            pltpu.VMEM((1, width), F32),
            pltpu.VMEM((1, width), F32),
            dma(9),
            pltpu.VMEM((columns, size, cols), F32),
            pltpu.VMEM((columns, depth, cols), BF16),
            pltpu.VMEM((2 * HEAD, width), F32),
            pltpu.VMEM((size, width), F32),
            pltpu.VMEM((10, size, width), BF16),
            pltpu.VMEM((2, size, width), BF16),
            pltpu.VMEM((size, width), F32),
            pltpu.VMEM((2, HEAD, width), BF16),
            pltpu.VMEM((HEAD, width), F32),
            pltpu.VMEM((2, HEAD, width), BF16),
            pltpu.VMEM((HEAD, width), F32),
            pltpu.VMEM((size, width), BF16),
            pltpu.VMEM((blocks, 2 * HEAD, wide), BF16),
            pltpu.VMEM((blocks, 2 * HEAD, wide), BF16),
            pltpu.VMEM((blocks, shares, HEAD, wide // shares), BF16),
            pltpu.VMEM((blocks, shares, HEAD, wide // shares), BF16),
            pltpu.SemaphoreType.DMA,
            dma(2),
            dma(others, 2, pieces),
            dma(others, 2, pieces),
            dma(others, pieces),
            dma(others, pieces),
            dma(others, pieces),
            dma(others, pieces),
            dma(others, 4, pieces),
            dma(others, 4, pieces),
            dma(blocks),
            dma(blocks),
            dma(blocks, shares),
            dma(blocks, shares),
        ],
        compiler_params=pltpu.CompilerParams(collective_id=0, has_side_effects=True, vmem_limit_bytes=45 * 2**20),
        name="fused_mixer",
    )(
        *map(pin, (q, key_rows[0], value_rows[0], decay_low[0], rate_low[0], decay_up, rate_up,
        decay_base[None], norm_gain[None], out_weight)),
    )
    return out[None]


def solution(mesh):
    in_specs = (
        P("dp", "sp", None),
        P("dp", "sp", None),
        P("dp", "sp", None),
        P("dp", "sp", None),
        P("dp", "sp", None),
        P(),
        P(),
        P(),
        P(),
        P(None, "dp"),
    )
    return jax.shard_map(
        functools.partial(per_device, mesh.shape["sp"], mesh.shape["dp"]),
        mesh=mesh, in_specs=in_specs, out_specs=P("dp", "sp", None), check_vma=False,
    )
```

```python
import functools
import math

import jax
import jax.numpy as jnp
from jax import lax
from jax.experimental import pallas as pl
from jax.experimental.pallas import tpu as pltpu
from jax.sharding import PartitionSpec as P

HEAD = 64
PAIR = 2 * HEAD
WIDE = 4
FINE = 16
FINE = 16

F32 = jnp.float32
BF16 = jnp.bfloat16


def mm(left, right):
    return lax.dot_general(left, right, (((1,), (0,)), ((), ())), preferred_element_type=F32)


def mm_nt(left, right):
    return lax.dot_general(left, right, (((1,), (1,)), ((), ())), preferred_element_type=F32)


def mm_tn(left, right):
    return lax.dot_general(left, right, (((0,), (0,)), ((), ())), preferred_element_type=F32)


def split(x):
    high = x.astype(BF16)
    return high, (x - high.astype(F32)).astype(BF16)


def mm_ab(left, right, form=mm):
    return form(left[0], right[0]) + form(left[0], right[1]) + form(left[1], right[0])


def beside(*parts):
    return jnp.concatenate(parts, axis=1)


def below(*parts):
    return jnp.concatenate(parts, axis=0)


def swap(x):
    return pltpu.roll(x, HEAD, 1)


def iota(shape, dim):
    return lax.broadcasted_iota(jnp.int32, shape, dim)


def first_half(shape):
    return iota(shape, len(shape) - 1) < HEAD


def stack_pair(x):
    here = lax.rem(iota(x.shape, 1), PAIR) < HEAD
    zero = jnp.zeros_like(x)
    return jnp.concatenate([jnp.where(here, x, zero), jnp.where(here, zero, x)], axis=0)


def head_ones(scale):
    row = iota((PAIR, PAIR), 0)
    col = iota((PAIR, PAIR), 1)
    return jnp.where(row // HEAD == col // HEAD, F32(scale), F32(0.0)).astype(BF16)


def head_sum(x, ones):
    return mm(beside(*split(x)), below(ones, ones))


def crossed(x, y):
    zero = jnp.zeros_like(x)
    return below(beside(x, zero), beside(zero, y))


def crossed(x, y):
    zero = jnp.zeros_like(x)
    return below(beside(x, zero), beside(zero, y))


def solve(parts, size):
    row = iota((size, size), 0)
    col = iota((size, size), 1)

    def picked(x, block):
        keep = (row // (2 * block) == col // (2 * block)) & (row // block != col // block)
        return jnp.where(keep, x, jnp.zeros_like(x))

    small = [jnp.where(row // FINE == col // FINE, z, 0.0) for z, _ in parts]
    block = 1
    while block < FINE:
        high = [x.astype(BF16) for x in small]
        steps = []
        for x, y in zip(high[::2], high[1::2]):
            both = mm(beside(picked(x, block), picked(y, block)), crossed(x, y))
            steps += [both[:, :size], both[:, size:]]
        small = [x - step for x, step in zip(small, steps)]
        block *= 2
    whole = []
    for (z, y), x in zip(parts, small):
        x = x.astype(BF16)
        both = beside(z, y)
        whole.append(both - mm(beside(x, x), below(*split(both))))
    while block < size:
        keep = (row // (2 * block) == col // (2 * block)) & (row // block != col // block)
        found = []
        for x in whole:
            first = size if 2 * block == size else 0
            moves, high, low, evens, odds = [], [], [], [], []
            for r in range(0, size, 2 * block):
                m, n = r + block, r + 2 * block
                z = x[m:n, :size].astype(BF16)
                moves.append(jnp.where(keep[m:n], z, jnp.zeros_like(z)))
                evens.append(x[r:m, first:])
                odds.append(x[m:n, first:])
                for parts_of, piece in zip((high, low), split(evens[-1])):
                    parts_of += [piece, jnp.zeros_like(piece)]
            move = below(*moves)
            step = mm(beside(move, move), below(*high, *low))
            rows = []
            for i, (even, odd) in enumerate(zip(evens, odds)):
                rows += [even, odd - step[i * block : (i + 1) * block]]
            found.append(below(*rows))
        whole = found
        block *= 2
    return whole


def gates(squashed, rate_low, decay_up, rate_up, base):
    decay_pre = (base + mm(squashed, decay_up)).astype(BF16).astype(F32)
    rate_pre = mm(rate_low, rate_up).astype(BF16).astype(F32)
    log_decay = -math.exp(-0.5) / (1.0 + jnp.exp(-decay_pre))
    rate = 1.0 / (1.0 + jnp.exp(-rate_pre))
    return log_decay, rate


def pair_grid(left, right):
    return mm_nt(beside(*left), beside(right[0], right[0])) + mm_nt(left[0], right[1])


def chunk_maps(pairs):
    size = pairs[0][0].shape[0]
    middle = size // 2
    row = iota((size, size), 0)
    col = iota((size, size), 1)
    strict = row > col
    upto = jnp.where(row >= col, F32(1.0), F32(0.0)).astype(BF16)
    upto = beside(upto, upto)
    ones = head_ones(1.0)
    half = first_half((size, PAIR))
    runs = [mm(upto, below(*split(p[2]))) for p in pairs]
    means = head_ones(1.0 / HEAD)
    sums = []
    values = []
    for p in pairs:
        k = p[0].astype(F32)
        sums.append(mm((k * k).astype(BF16), ones))
        values.append(split(p[1].astype(F32) - mm(p[1], means)))
    made = []
    for (k, v, log_decay, rate), running, total in zip(pairs, runs, sums):
        k = k.astype(F32)
        centre = running[middle : middle + 1]
        behind = jnp.exp(centre - running)
        unit = k * lax.rsqrt(1.0 + total)
        erase_from = unit * jnp.exp(running - log_decay - centre)
        made.append((erase_from, k * behind, unit * rate * behind, centre, running[size - 1 :]))
    grids = []
    keeps = []
    for erase_from, key_to, erase_to, _, _ in made:
        keeps.append(split(key_to) + split(erase_to))
        key_high, key_low, erase_high, erase_low = keeps[-1]
        right = below(key_high, erase_high), below(key_low, erase_low)
        grids.append(pair_grid(split(stack_pair(erase_from)), right))

    def part(grid, i, j):
        return jnp.where(
            strict, grid[i * size : (i + 1) * size, j * size : (j + 1) * size], 0.0
        )

    parts = []
    for v, grid, (erase_from, _, _, centre, _) in zip(values, grids, made):
        keys = split(beside(part(grid, 0, 0), part(grid, 1, 0)))
        carried = mm_ab(keys, [stack_pair(x) for x in v])
        erase = erase_from * jnp.exp(centre)
        parts.append((part(grid, 0, 1), jnp.where(half, erase, swap(carried))))
        parts.append((part(grid, 1, 1), jnp.where(half, swap(erase), carried)))
    solved = solve(parts, size)
    row2 = iota((PAIR, PAIR), 0)
    col2 = iota((PAIR, PAIR), 1)
    half2 = first_half((HEAD, PAIR))
    fold = lambda x: jnp.where(half2, x[:HEAD], x[HEAD:])
    out = []
    for i, (v, keep, running, (_, _, _, centre, final)) in enumerate(
        zip(values, keeps, runs, made)
    ):
        a, b = solved[2 * i], solved[2 * i + 1]
        both = split(beside(jnp.where(half, a, swap(b)), jnp.where(half, swap(a), b)))
        at_end = fold(jnp.transpose(jnp.broadcast_to(jnp.exp(final - centre), (PAIR, PAIR))))
        moved = mm_tn(below(*keep[2:]), below(both[0], both[0])) + mm_tn(keep[2], both[1])
        gained = mm_tn(below(*keep[:2]), below(v[0], v[0])) + mm_tn(keep[0], v[1])
        decay = jnp.where(row2 == col2, jnp.broadcast_to(jnp.exp(final), (PAIR, PAIR)), 0.0)
        transfer = fold(decay) - fold(moved[:, :PAIR]) * at_end
        added = fold(gained - moved[:, PAIR:]) * at_end
        halves = tuple(x[:, j : j + PAIR] for j in (0, PAIR) for x in both)
        out.append((transfer, added, running) + keep + halves + v)
    return out


def chunk_reads(pairs):
    size = pairs[0][0].shape[0]
    within = iota((size, size), 0) >= iota((size, size), 1)
    grids = []
    fronts = []
    for q, running, keep in pairs:
        centre = running[size // 2 : size // 2 + 1]
        read_from = q.astype(F32) * jnp.exp(running - centre)
        fronts.append(read_from * jnp.exp(centre))
        right = below(keep[0], keep[2]), below(keep[1], keep[3])
        grids.append(pair_grid(split(stack_pair(read_from)), right))
    out = []
    for (_, _, keep), grid, front in zip(pairs, grids, fronts):
        part = lambda i, j: jnp.where(
            within, grid[i * size : (i + 1) * size, j * size : (j + 1) * size], 0.0
        )
        read_keys = split(beside(part(0, 0), part(1, 0)))
        read_erase = split(beside(part(0, 1), part(1, 1)))
        here = mm_ab(read_keys, [stack_pair(x) for x in keep[8:]])
        both = [stack_pair(beside(keep[i + 4], keep[i + 6])) for i in (0, 1)]
        taken = mm_ab(read_erase, both)
        out.append(split(front - taken[:, :PAIR]) + (here - taken[:, PAIR:],))
    return out


def fused_kernel(devices, columns, wide, pieces, q_hbm, k_hbm, v_hbm, low_hbm, rate_hbm,
                 dup_hbm, rup_hbm, base_hbm, gain_hbm, weight_ref, out_ref, q_ref, k_ref, v_ref,
                 low_ref, rate_ref, dup_ref, rup_ref, base_ref, gain_ref, in_sem, sums_ref, weights,
                 own_ref,
                 running_ref, kept_ref, read_ref, here_ref, first_ref, first_add, both_ref, both_add,
                 mix_ref, give_buf, take_buf, start_buf, end_buf, own_sem, near_sem, far_send,
                 far_recv, side_send, side_recv, long_send, long_recv, pass_send, pass_recv,
                 give_send, give_recv, send_sem, recv_sem):
    me = lax.axis_index("sp")
    mine = lax.axis_index("dp")
    partner = mine + 1 - 2 * lax.rem(mine, 2)
    odd = lax.rem(me, 2)
    pair = me // 2
    side = me + 1 - 2 * odd
    long = me + 2 - 4 * lax.rem(pair, 2)
    width = q_ref.shape[1]
    blocks = width // wide
    chain = devices // 2
    others = columns // 2 - 1
    cols = weight_ref.shape[1]
    piece = weight_ref.shape[0] // (4 * pieces)
    has_left = pair > 0
    has_right = pair < chain - 1
    barrier = pltpu.get_barrier_semaphore()

    def greet(where):
        pl.semaphore_signal(barrier, inc=1, device_id=where, device_id_type=pl.DeviceIdType.MESH)

    def ahead_of(j):
        return lax.rem(mine + 2 * (j + 1), columns)

    def behind_of(j):
        return lax.rem(mine + columns - 2 * (j + 1), columns)

    def remote(src, dst, send, recv, where):
        return pltpu.make_async_remote_copy(
            src_ref=src, dst_ref=dst, send_sem=send, recv_sem=recv,
            device_id=where, device_id_type=pl.DeviceIdType.MESH,
        )

    inputs = [
        (low_hbm, low_ref), (rate_hbm, rate_ref), (base_hbm, base_ref), (dup_hbm, dup_ref),
        (rup_hbm, rup_ref), (k_hbm, k_ref), (v_hbm, v_ref), (q_hbm, q_ref), (gain_hbm, gain_ref),
    ]
    loads = [pltpu.make_async_copy(x, y, in_sem.at[i]) for i, (x, y) in enumerate(inputs)]
    for load in loads:
        load.start()
    greet({"dp": partner})
    greet({"sp": side})
    for j in range(others):
        greet({"dp": ahead_of(j)})

    @pl.when(has_left)
    def _():
        greet({"sp": me - 2})

    @pl.when(has_right)
    def _():
        greet({"sp": me + 2})

    own = pltpu.make_async_copy(weight_ref, weights.at[mine], own_sem)
    pl.semaphore_wait(
        barrier, 2 + others + jnp.minimum(pair, 1) + jnp.minimum(chain - 1 - pair, 1)
    )

    quarter = lax.rem(me, 4)
    side_quarter = quarter + 1 - 2 * odd
    long_quarter = lax.rem(quarter + 2, 4)
    last_quarter = 3 - quarter
    arrivals = (quarter, last_quarter, side_quarter, long_quarter)

    def rows(part, c):
        return pl.ds((part * pieces + c) * piece, piece)

    def far(j, part, c):
        at = rows(arrivals[part], c)
        return remote(
            weight_ref.at[at], weights.at[mine, at],
            far_send.at[j, part, c], far_recv.at[j, part, c], {"dp": ahead_of(j)},
        )

    def spread(j, c, send, recv, where):
        at = rows(quarter, c)
        spot = weights.at[behind_of(j), at]
        return remote(spot, spot, send.at[j, c], recv.at[j, c], {"sp": where})

    def aside(j, c):
        return spread(j, c, side_send, side_recv, side)

    def along(j, c):
        return spread(j, c, long_send, long_recv, long)

    def passed(j, part, c):
        spot = weights.at[behind_of(j), rows(arrivals[part], c)]
        return remote(
            spot, spot, pass_send.at[j, part, c], pass_recv.at[j, part, c], {"dp": partner},
        )

    near = remote(weight_ref, weights.at[mine], near_sem.at[0], near_sem.at[1], {"dp": partner})
    for part in range(2):
        for c in range(pieces):
            for j in range(others):
                far(j, part, c).start()

    def forward(part, c):
        for j in range(others):
            if part < 2:
                far(j, part, c).wait_recv()
            elif part == 2:
                aside(j, c).wait_recv()
            else:
                along(j, c).wait_recv()
            if part == 0:
                along(j, c).start()
            passed(j, part, c).start()

    def lend(c):
        for j in range(others):
            aside(j, c).start()

    def lanes_of(g):
        return pl.ds(pl.multiple_of(g * wide, wide), wide)

    def cut(x, i):
        return x[:, i * PAIR : (i + 1) * PAIR]

    def cuts(x):
        return [cut(x, i) for i in range(wide // PAIR)]

    def give(b):
        return remote(
            give_buf.at[b], take_buf.at[b], give_send.at[b], give_recv.at[b], {"sp": side}
        )

    def copy(b, i):
        return remote(
            end_buf.at[b, i], start_buf.at[b, i], send_sem.at[b, i], recv_sem.at[b, i],
            {"sp": lax.rem(me + 2, devices)},
        )

    shares = end_buf.shape[1]
    share = wide // shares

    def start_of(b):
        return beside(*[start_buf[b, i] for i in range(shares)])

    def make(b):
        at = lanes_of(b)
        squashed = jnp.tanh(low_ref[...].astype(F32)).astype(BF16)
        log_decay, rate = gates(
            squashed, rate_ref[...], dup_ref[:, at], rup_ref[:, at], base_ref[:, at]
        )
        pairs = list(zip(*map(cuts, (k_ref[:, at], v_ref[:, at], log_decay, rate))))
        parts = [beside(*part) for part in zip(*chunk_maps(pairs))]
        maps = below(parts[0], parts[1])
        own_ref[:, at] = maps
        give_buf[b] = maps.astype(BF16)
        running_ref[:, at] = parts[2]
        for i, part in enumerate(parts[3:]):
            kept_ref[i, :, at] = part
        give(b).start()

    def combine(b):
        at = lanes_of(b)
        give(b).wait_recv()
        own, taken = own_ref[:, at], take_buf[b].astype(F32)
        is_odd = iota(own.shape, 0) * 0 + odd == 1
        first, second = jnp.where(is_odd, taken, own), jnp.where(is_odd, own, taken)
        found = []
        for x, y in zip(cuts(first), cuts(second)):
            left = split(y[:HEAD])
            right = split(beside(stack_pair(x[:HEAD]), stack_pair(x[HEAD:])))
            found.append((mm_ab(left, right), y[HEAD:]))
        both = beside(*[x[:, :PAIR] for x, _ in found])
        added = beside(*[x[:, PAIR:] + y for x, y in found])
        both_ref[0, :, at], both_ref[1, :, at] = split(both)
        both_add[:, at] = added
        same = (iota((HEAD, wide), 1) % HEAD == iota((HEAD, wide), 0)).astype(F32)
        is_odd = is_odd[:HEAD]
        first_ref[0, :, at], first_ref[1, :, at] = split(jnp.where(is_odd, first[:HEAD], same))
        first_add[:, at] = jnp.where(is_odd, first[HEAD:], 0.0)

        @pl.when(jnp.logical_not(has_left) & has_right)
        def _():
            for i in range(shares):
                end_buf[b, i] = added[:, i * share : (i + 1) * share].astype(BF16)
                copy(b, i).start()

    def apply(high, low, state):
        return mm(beside(high, low), below(state, state))

    def advance(b):
        for i in range(shares):
            copy(b, i).wait_recv()

            @pl.when(has_right)
            def _():
                at = pl.ds(pl.multiple_of(b * wide + i * share, share), share)
                high, low, start = both_ref[0, :, at], both_ref[1, :, at], start_buf[b, i]
                ends = []
                for j in range(share // PAIR):
                    h, l, x = cut(high, j), cut(low, j), cut(start, j)
                    ends.append(apply(h, l, stack_pair(x)))
                end_buf[b, i] = (beside(*ends) + both_add[:, at]).astype(BF16)
                copy(b, i).start()

    def prepare(b):
        at = lanes_of(b)
        kept = [cuts(kept_ref[j, :, at]) for j in range(kept_ref.shape[0])]
        keeps = list(zip(*kept))
        pairs = list(zip(*map(cuts, (q_ref[:, at], running_ref[:, at])), keeps))
        high, low, here = [beside(*part) for part in zip(*chunk_reads(pairs))]
        read_ref[0, :, at], read_ref[1, :, at], here_ref[:, at] = high, low, here

    ones = head_ones(1.0 / HEAD)

    def read(b):
        at = lanes_of(b)
        high, low, start = first_ref[0, :, at], first_ref[1, :, at], start_of(b)
        starts = [apply(h, l, stack_pair(x)) for h, l, x in zip(*map(cuts, (high, low, start)))]
        starts = [split(x + y) for x, y in zip(starts, cuts(first_add[:, at]))]
        high, low, here = read_ref[0, :, at], read_ref[1, :, at], here_ref[:, at]
        reads = []
        for h, l, x, (s_high, s_low) in zip(*map(cuts, (high, low, here)), starts):
            reads.append(apply(h, l, stack_pair(s_high)) + mm(h, stack_pair(s_low)) + x)
        spans = [head_sum(x * x, ones) for x in reads]
        mix = beside(*[x * lax.rsqrt(y + 1.0) for x, y in zip(reads, spans)])
        mix = (mix * gain_ref[:, at]).astype(BF16)
        mix_ref[:, at] = mix
        for i, d in enumerate((mine, partner)):
            sums_ref[i] += mm(mix, weights[d, at])

    @pl.when(jnp.logical_not(has_left))
    def _():
        start_buf[...] = jnp.zeros_like(start_buf)

    sums_ref[:2] = jnp.zeros((2, *sums_ref.shape[1:]), F32)
    for load in loads:
        load.wait()
    own.start()
    near.start()

    lag = jnp.maximum(pair - 1, 0)
    slots = 2 * blocks + max(chain - 2, 0)
    plan = [
        (1, [(0, 0)]),
        (2, [(0, 1)]),
        (blocks - 1, [(-1, 0), (-1, 1), (0, 2)]),
    ]
    early = [
        (blocks + 1, [(0, 3), (-1, 2), (-1, 3)]),
        (2 * blocks, [(3, 0), (3, 1), (2, 0), (3, 2), (2, 1), (1, 0)]),
    ]
    done = [x for at, todo in plan + early if at < slots - 1 for x in todo]
    head = (blocks - 1) * wide
    far_columns = [
        d for j in range(others)
        for d in (behind_of(j), lax.rem(partner + columns - 2 * (j + 1), columns))
    ]

    def slot(s, carry):
        def pump(which):
            for at, todo in [x for x in which if x[0] < slots - 1]:
                @pl.when(s == at)
                def _():
                    for part, c in todo:
                        (lend if part < 0 else functools.partial(forward, part))(c)

        pump(early)

        @pl.when(s == slots - 1)
        def _():
            for c in range(pieces):
                for part in (3, 2, 1, 0):
                    if (part, c) not in done:
                        forward(part, c)
            for i, d in enumerate(far_columns):
                if i % 2 == 1:
                    for part in range(4):
                        for c in range(pieces):
                            passed(i // 2, part, c).wait_recv()
                sums_ref[2 + i] = mm(mix_ref[:, :head], weights[d, :head])

        @pl.when(s < blocks)
        def _():
            make(s)

        @pl.when(((s >= 1) & (s < blocks)) | (s == 2 * blocks - 1))
        def _():
            combine(jnp.minimum(s, blocks) - 1)

        b = s - blocks - lag
        live = (b >= 0) & (b < blocks)

        @pl.when(live & has_left)
        def _():
            advance(b)

        @pl.when((s >= blocks) & (s < 2 * blocks))
        def _():
            prepare(s - blocks)

        @pl.when(s == blocks)
        def _():
            own.wait()
            near.wait_recv()

        @pl.when(live)
        def _():
            read(b)

        pump(plan)
        return carry

    lax.fori_loop(0, slots, slot, 0)
    def columns_of(d):
        return pl.ds(pl.multiple_of(d * cols, cols), cols)

    for i, d in enumerate((mine, partner)):
        out_ref[:, columns_of(d)] = sums_ref[i].astype(BF16)
    for i, d in enumerate(far_columns):
        rest = mm(mix_ref[:, head:], weights[d, head:])
        out_ref[:, columns_of(d)] = (sums_ref[2 + i] + rest).astype(BF16)

    near.wait_send()
    for j in range(others):
        for part in range(4):
            for c in range(pieces):
                passed(j, part, c).wait_send()
        for c in range(pieces):
            aside(j, c).wait_send()
            along(j, c).wait_send()
            far(j, 0, c).wait_send()
            far(j, 1, c).wait_send()

    for b in range(blocks):
        give(b).wait_send()

    @pl.when(has_right)
    def _():
        for b in range(blocks):
            for i in range(shares):
                copy(b, i).wait_send()


def pin(x):
    return pltpu.with_memory_space_constraint(x, pltpu.HBM)


def per_device(devices, columns, query_rows, key_rows, value_rows, decay_low, rate_low, decay_up,
               rate_up, decay_base, norm_gain, out_weight):
    q = query_rows[0]
    size, width = q.shape
    depth, cols = out_weight.shape
    wide = PAIR * math.gcd(width // PAIR, WIDE)
    blocks = width // wide
    shares = math.gcd(wide // PAIR, 2)
    pieces = 4
    others = columns // 2 - 1
    vmem = pl.BlockSpec(memory_space=pltpu.VMEM)
    dma = lambda *dims: pltpu.SemaphoreType.DMA(dims)
    out = pl.pallas_call(
        functools.partial(fused_kernel, devices, columns, wide, pieces),
        in_specs=[pl.BlockSpec(memory_space=pl.ANY)] * 10,
        out_specs=vmem,
        out_shape=jax.ShapeDtypeStruct((size, columns * cols), BF16),
        scratch_shapes=[
            pltpu.VMEM((size, width), BF16),
            pltpu.VMEM((size, width), BF16),
            pltpu.VMEM((size, width), BF16),
            pltpu.VMEM(decay_low.shape[1:], BF16),
            pltpu.VMEM(rate_low.shape[1:], BF16),
            pltpu.VMEM(decay_up.shape, BF16),
            pltpu.VMEM(rate_up.shape, BF16),
            pltpu.VMEM((1, width), F32),
            pltpu.VMEM((1, width), F32),
            dma(9),
            pltpu.VMEM((columns, size, cols), F32),
            pltpu.VMEM((columns, depth, cols), BF16),
            pltpu.VMEM((2 * HEAD, width), F32),
            pltpu.VMEM((size, width), F32),
            pltpu.VMEM((10, size, width), BF16),
            pltpu.VMEM((2, size, width), BF16),
            pltpu.VMEM((size, width), F32),
            pltpu.VMEM((2, HEAD, width), BF16),
            pltpu.VMEM((HEAD, width), F32),
            pltpu.VMEM((2, HEAD, width), BF16),
            pltpu.VMEM((HEAD, width), F32),
            pltpu.VMEM((size, width), BF16),
            pltpu.VMEM((blocks, 2 * HEAD, wide), BF16),
            pltpu.VMEM((blocks, 2 * HEAD, wide), BF16),
            pltpu.VMEM((blocks, shares, HEAD, wide // shares), BF16),
            pltpu.VMEM((blocks, shares, HEAD, wide // shares), BF16),
            pltpu.SemaphoreType.DMA,
            dma(2),
            dma(others, 2, pieces),
            dma(others, 2, pieces),
            dma(others, pieces),
            dma(others, pieces),
            dma(others, pieces),
            dma(others, pieces),
            dma(others, 4, pieces),
            dma(others, 4, pieces),
            dma(blocks),
            dma(blocks),
            dma(blocks, shares),
            dma(blocks, shares),
        ],
        compiler_params=pltpu.CompilerParams(collective_id=0, has_side_effects=True, vmem_limit_bytes=45 * 2**20),
        name="fused_mixer",
    )(
        *map(pin, (q, key_rows[0], value_rows[0], decay_low[0], rate_low[0], decay_up, rate_up,
        decay_base[None], norm_gain[None], out_weight)),
    )
    return out[None]


def solution(mesh):
    in_specs = (
        P("dp", "sp", None),
        P("dp", "sp", None),
        P("dp", "sp", None),
        P("dp", "sp", None),
        P("dp", "sp", None),
        P(),
        P(),
        P(),
        P(),
        P(None, "dp"),
    )
    return jax.shard_map(
        functools.partial(per_device, mesh.shape["sp"], mesh.shape["dp"]),
        mesh=mesh, in_specs=in_specs, out_specs=P("dp", "sp", None), check_vma=False,
    )
```
